256 devices in a mesh: kv: 16 (over y, x), tp: 16 (over z, core).
Axes of the slice: x: 4, y: 4, z: 8, core: 2. Of those that a mesh axis runs over, the one named last changes fastest.
Arguments:
- tokens: bfloat16 [256, 4096], P('kv', 'tp'), may hold values from -6 to 6
- attn_gain: float32 [4096], replicated, may hold values from 0.1 to 1.9
- w_query: bfloat16 [4096, 2048], P(None, 'tp'), may hold values from -0.09375 to 0.09375
- w_key: bfloat16 [4096, 2048], P(None, 'tp'), may hold values from -0.09375 to 0.09375
- w_value: bfloat16 [4096, 2048], P(None, 'tp'), may hold values from -0.09375 to 0.09375
- w_outgate: bfloat16 [4096, 2048], P(None, 'tp'), may hold values from -0.09375 to 0.09375
- w_rates: bfloat16 [2, 4096, 16], P(None, None, 'tp'), may hold values from -0.09375 to 0.09375
- head_rate: float32 [16], P('tp'), may hold values from 0.02 to 2
- head_gain: float32 [2048], P('tp'), may hold values from 0.1 to 1.9
- w_out: bfloat16 [2048, 4096], P('tp'), may hold values from -0.125 to 0.125
- state: float32 [256, 16, 128, 128], P('kv', 'tp'), may hold values from -2.4 to 2.4
- mlp_gain: float32 [4096], replicated, may hold values from 0.1 to 1.9
- w_gate: bfloat16 [4096, 11264], P(None, ('kv', 'tp')), may hold values from -0.09375 to 0.09375
- w_up: bfloat16 [4096, 11264], P(None, ('kv', 'tp')), may hold values from -0.09375 to 0.09375
- w_down: bfloat16 [4096, 11264], P(None, ('kv', 'tp')), may hold values from -0.25 to 0.25
Outputs:
- result: bfloat16 [256, 4096], P('kv', 'tp')
- new_state: float32 [256, 16, 128, 128], P('kv', 'tp')
The draws below stay inside these ranges and needn't reach their ends.
All inputs are finite; a program needn't handle non-finite values.
Results may differ from the reference program's by a relative error of at most 0.014.
Values may be sent and summed in bfloat16 or wider, within the bound.
No kernel may reach another device: no remote copies, remote signals or barrier semaphores. Data moves between devices by JAX's collectives and lax.ppermute only.
A program may use at most 64 MiB of HBM per device.

```python
import math
import jax
import jax.numpy as jnp
from jax import lax

D = 4096
H = 16
HEAD = 128
FF = 11264
BATCH = 256


def with_spikes(entries, key, source, target, shards_of, factor):
    owner, partner = [(jnp.arange(entries.shape[axis_at]) // (entries.shape[axis_at] // shards_of)).reshape([-1 if axis == axis_at else 1 for axis in range(entries.ndim)]) for axis_at in (source, target)]
    chosen = jax.random.permutation(key, shards_of)[partner]
    strong = (owner == chosen) | (owner == (partner + shards_of // 2) % shards_of)
    return jnp.where(strong, factor * entries, entries)


def shard_levels(key, shape, cuts, least, top_value):
    level = 1.0
    for axis_at, parts in cuts:
        steps = jax.random.uniform(jax.random.fold_in(jax.random.fold_in(key, 6), axis_at), (parts,), jnp.float32, least / len(cuts), top_value / len(cuts))
        level = level * jnp.repeat(jnp.exp(steps), shape[axis_at] // parts).reshape((-1,) + (1,) * (len(shape) - 1 - axis_at))
    return level


def scatter_about(key, dims, width, reach, shards=(), kind=jnp.bfloat16):
    array = jax.random.normal(key, dims, jnp.float32) * width
    if len(shards) > 0:
        array = shard_levels(key, dims, shards, -0.22, 0.18) * array
    return jnp.clip(array, min=-reach, max=reach).astype(kind)


def heavy_noise(key, dims, width, most, split, heavy, dtype=jnp.bfloat16):
    array = width * jax.random.normal(key, dims, jnp.float32)
    if split:
        array = array * shard_levels(key, dims, split, -0.22, 0.18)
    return jnp.clip(with_spikes(array, jax.random.fold_in(key, 3), *heavy), -most, most).astype(dtype)


def setup_inputs(seed: int = 0) -> dict:
    splits = jax.random.split(jax.random.key(seed), 16)
    return {
        "tokens": scatter_about(splits[0], (BATCH, D), 1.0, 6.0, ((0, 16), (1, 16))),
        "attn_gain": jnp.clip(1.0 + 0.18 * jax.random.normal(splits[1], (D,), jnp.float32), 0.1, 1.9),
        "w_query": scatter_about(splits[2], (D, H * HEAD), D ** -0.5, 0.09375, ((1, 16),)),
        "w_key": scatter_about(splits[3], (D, H * HEAD), D ** -0.5, 0.09375, ((1, 16),)),
        "w_value": scatter_about(splits[4], (D, H * HEAD), D ** -0.5, 0.09375, ((1, 16),)),
        "w_outgate": scatter_about(splits[5], (D, H * HEAD), D ** -0.5, 0.09375, ((1, 16),)),
        "w_rates": scatter_about(splits[6], (2, D, H), D ** -0.5, 0.09375, ((2, 16),)),
        "head_rate": jnp.clip(jnp.exp(math.log(2.0) - 4.6051702 * jax.random.uniform(splits[7], (H,), jnp.float32) ** shard_levels(splits[7], (H,), ((0, 16),), -0.2, 0.2)), 0.02, 2.0),
        "head_gain": jnp.clip(1.0 + 0.18 * jax.random.normal(splits[8], (H * HEAD,), jnp.float32), 0.1, 1.9),
        "w_out": scatter_about(splits[9], (H * HEAD, D), (H * HEAD) ** -0.5, 0.125, ((0, 16),)),
        "state": scatter_about(splits[10], (BATCH, H, HEAD, HEAD), 0.3, 2.4, ((0, 16), (1, 16)), jnp.float32),
        "mlp_gain": jnp.clip(1.0 + 0.18 * jax.random.normal(splits[11], (D,), jnp.float32), 0.1, 1.9),
        "w_gate": scatter_about(splits[12], (D, FF), D ** -0.5, 0.09375, ((1, 256),)),
        "w_up": scatter_about(splits[13], (D, FF), D ** -0.5, 0.09375, ((1, 256),)),
        "w_down": heavy_noise(splits[14], (D, FF), FF ** -0.5, 0.25, ((1, 256),), (1, 0, 256, 6.0)),
    }


EPS = 1e-06

def row_norm(values, gain):
    floats = values.astype(jnp.float32)
    scaled = floats * lax.rsqrt(lax.optimization_barrier(jnp.mean(floats * floats, axis=-1, keepdims=True)) + EPS)
    return (scaled * gain.astype(jnp.float32)).astype(jnp.bfloat16)

def reference(tokens, attn_gain, w_query, w_key, w_value, w_outgate, w_rates, head_rate, head_gain, w_out, state, mlp_gain, w_gate, w_up, w_down):
    count = tokens.shape[0]
    normed = row_norm(tokens, attn_gain)
    query = jnp.dot(normed, w_query, preferred_element_type=jnp.float32).reshape(count, H, HEAD)
    key = jnp.dot(normed, w_key, preferred_element_type=jnp.float32).reshape(count, H, HEAD)
    value = jnp.dot(normed, w_value, preferred_element_type=jnp.float32).reshape(count, H, HEAD)
    gate_in = jnp.dot(normed, w_outgate, preferred_element_type=jnp.float32).reshape(count, H, HEAD)
    write_raw = jnp.dot(normed, w_rates[0], preferred_element_type=jnp.float32)
    decay_raw = jnp.dot(normed, w_rates[1], preferred_element_type=jnp.float32)
    unit_query = query * lax.rsqrt(lax.optimization_barrier(jnp.sum(query * query, axis=-1, keepdims=True)) + EPS) * HEAD ** (-0.5)
    unit_key = key * lax.rsqrt(lax.optimization_barrier(jnp.sum(key * key, axis=-1, keepdims=True)) + EPS)
    strength = jax.nn.sigmoid(write_raw)
    fade = jnp.exp(-head_rate * jax.nn.softplus(decay_raw))
    carried = state * fade[:, :, None, None]
    fresh = strength[:, :, None] * (value - jnp.einsum('bhi,bhiv->bhv', unit_key, carried))
    new_state = carried + unit_key[:, :, :, None] * fresh[:, :, None, :]
    readout = jnp.einsum('bhi,bhiv->bhv', unit_query, new_state)
    normed_out = readout * lax.rsqrt(lax.optimization_barrier(jnp.mean(readout * readout, axis=-1, keepdims=True)) + EPS)
    mixed = (normed_out * head_gain.reshape(H, HEAD) * jax.nn.silu(gate_in)).astype(jnp.bfloat16).reshape(count, H * HEAD)
    projected = jnp.dot(mixed, w_out, preferred_element_type=jnp.float32)
    residual = (tokens.astype(jnp.float32) + projected).astype(jnp.bfloat16)
    normed_mlp = row_norm(residual, mlp_gain)
    gate_pre = jnp.dot(normed_mlp, w_gate, preferred_element_type=jnp.float32)
    up_pre = jnp.dot(normed_mlp, w_up, preferred_element_type=jnp.float32)
    hidden = (jax.nn.silu(gate_pre) * up_pre).astype(jnp.bfloat16)
    down = lax.dot_general(hidden, w_down, (((1,), (1,)), ((), ())), preferred_element_type=jnp.float32)
    result = (residual.astype(jnp.float32) + down).astype(jnp.bfloat16)
    return (result, new_state)
```

```python
import jax
import jax.numpy as jnp
from jax import lax
from jax.sharding import PartitionSpec as P

EPS = 1e-06
UNITS = 48


def y_ring(shift, side):
    return [
        (side * y + x, side * ((y + shift) % side) + x) for y in range(side) for x in range(side)
    ]


def plane_groups(side, tp):
    return [[(side * y + x) * tp + t for x in range(side) for t in range(tp)] for y in range(side)]


def body(
    tokens,
    attn_gain,
    w_query,
    w_key,
    w_value,
    w_outgate,
    w_rates,
    head_rate,
    head_gain,
    w_out,
    state,
    mlp_gain,
    w_gate,
    w_up,
    w_down,
):
    f32, bf16 = jnp.float32, jnp.bfloat16
    count, part = tokens.shape
    tp = lax.axis_size("tp")
    side = 4
    width = part * tp
    size = w_query.shape[1]
    units = w_gate.shape[1]

    own = jnp.stack([w_gate.T, w_up.T, w_down.T])
    own = jnp.pad(own, ((0, 0), (0, UNITS - units), (0, 0)))
    above = lax.ppermute(own, "kv", y_ring(1, side))
    below = lax.ppermute(own, "kv", y_ring(-1, side))

    tiles = lax.all_to_all(
        jnp.broadcast_to(tokens[None], (tp, count, part)), "tp", 0, 0, tiled=True
    )
    rows = jnp.moveaxis(tiles, 0, 1).reshape(count, width).astype(f32)
    scale = lax.rsqrt(jnp.mean(rows * rows, axis=-1, keepdims=True) + EPS)
    normed = (rows * scale * attn_gain).astype(bf16)
    query = jnp.dot(normed, w_query, preferred_element_type=f32)
    key = jnp.dot(normed, w_key, preferred_element_type=f32)
    value = jnp.dot(normed, w_value, preferred_element_type=f32)
    gate_in = jnp.dot(normed, w_outgate, preferred_element_type=f32)
    rates = jnp.einsum("bd,sdh->sbh", normed, w_rates, preferred_element_type=f32)
    unit_query = query * lax.rsqrt(jnp.sum(query * query, -1, keepdims=True) + EPS) * size**-0.5
    unit_key = key * lax.rsqrt(jnp.sum(key * key, -1, keepdims=True) + EPS)
    strength = jax.nn.sigmoid(rates[0])
    fade = jnp.exp(-head_rate * jax.nn.softplus(rates[1]))
    carried = state[:, 0] * fade[:, :, None]
    fresh = strength * (value - jnp.einsum("bi,biv->bv", unit_key, carried))
    new_state = carried + unit_key[:, :, None] * fresh[:, None, :]
    readout = jnp.einsum("bi,biv->bv", unit_query, new_state)
    normed_out = readout * lax.rsqrt(jnp.mean(readout * readout, -1, keepdims=True) + EPS)
    mixed = (normed_out * head_gain * jax.nn.silu(gate_in)).astype(bf16)
    partial = jnp.dot(mixed, w_out, preferred_element_type=f32).astype(bf16)
    tiles = jnp.moveaxis(partial.reshape(count, tp, part), 1, 0)
    tiles = lax.all_to_all(tiles, "tp", 0, 0, tiled=True)
    residual = (tokens.astype(f32) + jnp.sum(tiles.astype(f32), axis=0)).astype(bf16)

    residual, above, below = lax.optimization_barrier((residual, above, below))
    half = UNITS // 2
    far_low = lax.ppermute(above[:, :half], "kv", y_ring(1, side))
    far_high = lax.ppermute(below[:, half:], "kv", y_ring(-1, side))

    groups = plane_groups(side, tp)
    peers = side * tp
    tiles = lax.all_to_all(
        jnp.broadcast_to(residual[None], (peers, count, part)),
        ("kv", "tp"),
        0,
        0,
        tiled=True,
        axis_index_groups=groups,
    )
    rows = jnp.transpose(tiles.reshape(side, tp, count, part), (0, 2, 1, 3))
    rows = rows.reshape(side * count, width).astype(f32)
    scale = lax.rsqrt(jnp.mean(rows * rows, axis=-1, keepdims=True) + EPS)
    normed_mlp = (rows * scale * mlp_gain).astype(bf16)
    normed_mlp, far_low, far_high = lax.optimization_barrier((normed_mlp, far_low, far_high))
    weights = jnp.concatenate([own, above, below, far_low, far_high], axis=1)
    nt = (((1,), (1,)), ((), ()))
    gate_pre = lax.dot_general(normed_mlp, weights[0], nt, preferred_element_type=f32)
    up_pre = lax.dot_general(normed_mlp, weights[1], nt, preferred_element_type=f32)
    hidden = (jax.nn.silu(gate_pre) * up_pre).astype(bf16)
    partial = jnp.dot(hidden, weights[2], preferred_element_type=f32).astype(bf16)
    tiles = jnp.transpose(partial.reshape(side, count, tp, part), (0, 2, 1, 3))
    tiles = lax.all_to_all(
        tiles.reshape(peers, count, part),
        ("kv", "tp"),
        0,
        0,
        tiled=True,
        axis_index_groups=groups,
    )
    down = jnp.sum(tiles.astype(f32), axis=0)
    result = (residual.astype(f32) + down).astype(bf16)
    return (result, new_state[:, None])


def solution(mesh):
    return jax.shard_map(
        body,
        mesh=mesh,
        in_specs=(
            P("kv", "tp"),
            P(),
            P(None, "tp"),
            P(None, "tp"),
            P(None, "tp"),
            P(None, "tp"),
            P(None, None, "tp"),
            P("tp"),
            P("tp"),
            P("tp", None),
            P("kv", "tp", None, None),
            P(),
            P(None, ("kv", "tp")),
            P(None, ("kv", "tp")),
            P(None, ("kv", "tp")),
        ),
        out_specs=(P("kv", "tp"), P("kv", "tp", None, None)),
        check_vma=False,
    )
```

```python
import functools

import jax
import jax.numpy as jnp
from jax import lax
from jax.experimental import pallas as pl
from jax.experimental.pallas import tpu as pltpu
from jax.sharding import PartitionSpec as P


EPS = 1e-06
UNITS = 48
F32, BF16 = jnp.float32, jnp.bfloat16
NT = (((1,), (1,)), ((), ()))
VMEM = pl.BlockSpec(memory_space=pltpu.VMEM)
SMEM = pl.BlockSpec(memory_space=pltpu.SMEM)
HBM = pl.BlockSpec(memory_space=pltpu.HBM)


def in_vmem(*arrays):
    return [pltpu.with_memory_space_constraint(a, pltpu.VMEM) for a in arrays]


def y_ring(shift, side):
    return [
        (side * y + x, side * ((y + shift) % side) + x) for y in range(side) for x in range(side)
    ]


def plane_groups(side, tp):
    return [[(side * y + x) * tp + t for x in range(side) for t in range(tp)] for y in range(side)]


def silu(t):
    return t / (1.0 + jnp.exp(-t))


def norm_rows(tiles_ref, first, n_tiles, gain_ref, out_ref, at):
    rows, part = tiles_ref.shape[1:]
    total = jnp.zeros((rows, part), F32)
    for t in range(n_tiles):
        tile = tiles_ref[first + t].astype(F32)
        total = total + tile * tile
    mean = jnp.sum(total, axis=-1, keepdims=True) * (1.0 / (n_tiles * part))
    scale = lax.rsqrt(mean + EPS)
    for t in range(n_tiles):
        cols = slice(t * part, (t + 1) * part)
        tile = tiles_ref[first + t].astype(F32)
        out_ref[at : at + rows, cols] = (tile * scale * gain_ref[0:1, cols]).astype(BF16)


def attention_kernel(
    tiles_ref, gain_ref, wq_ref, wk_ref, wv_ref, wg_ref, wr_ref, rate_ref, head_gain_ref,
    wo_ref, state_ref, out_ref, new_state_ref, xn_ref, u_ref, w_ref,
):
    tp, count, part = tiles_ref.shape
    size = wq_ref.shape[1]
    norm_rows(tiles_ref, 0, tp, gain_ref, xn_ref, 0)
    xn = xn_ref[...]
    query = jnp.dot(xn, wq_ref[...], preferred_element_type=F32)
    key = jnp.dot(xn, wk_ref[...], preferred_element_type=F32)
    rates = lax.dot_general(xn, wr_ref[...], NT, preferred_element_type=F32)
    q = query * lax.rsqrt(jnp.sum(query * query, -1, keepdims=True) + EPS) * size**-0.5
    k = key * lax.rsqrt(jnp.sum(key * key, -1, keepdims=True) + EPS)
    q_high, k_high = q.astype(BF16), k.astype(BF16)
    q_low = (q - q_high.astype(F32)).astype(BF16)
    k_low = (k - k_high.astype(F32)).astype(BF16)
    probes = jnp.concatenate([k_high, k_low, q_high, q_low], axis=0)
    for b in range(count):
        read = jnp.dot(probes, state_ref[b].astype(BF16), preferred_element_type=F32)
        u_ref[b : b + 1, :] = read[b : b + 1] + read[count + b : count + b + 1]
        w_ref[b : b + 1, :] = read[2 * count + b : 2 * count + b + 1] + read[
            3 * count + b : 3 * count + b + 1
        ]
    value = jnp.dot(xn, wv_ref[...], preferred_element_type=F32)
    gate_in = jnp.dot(xn, wg_ref[...], preferred_element_type=F32)
    strength = 1.0 / (1.0 + jnp.exp(-rates[:, 0:1]))
    decay = rates[:, 1:2]
    softplus = jnp.maximum(decay, 0.0) + jnp.log(1.0 + jnp.exp(-jnp.abs(decay)))
    fade = jnp.exp(-rate_ref[...] * softplus)
    fresh = strength * (value - fade * u_ref[...])
    readout = fade * w_ref[...] + jnp.sum(q * k, -1, keepdims=True) * fresh
    scale = lax.rsqrt(jnp.mean(readout * readout, -1, keepdims=True) + EPS)
    mixed = (readout * scale * head_gain_ref[...] * silu(gate_in)).astype(BF16)
    for t in range(tp):
        cols = slice(t * part, (t + 1) * part)
        out_ref[t] = jnp.dot(mixed, wo_ref[:, cols], preferred_element_type=F32).astype(BF16)
    k_columns = k.T
    fade_rows = jnp.broadcast_to(fade, (count, size))
    for b in range(count):
        new_state_ref[b] = (
            fade_rows[b : b + 1, :] * state_ref[b]
            + k_columns[:, b : b + 1] * fresh[b : b + 1, :]
        )


def residual_kernel(tiles_ref, tokens_ref, out_ref, blocks_ref):
    total = tokens_ref[...].astype(F32)
    for t in range(tiles_ref.shape[0]):
        total = total + tiles_ref[t].astype(F32)
    residual = total.astype(BF16)
    out_ref[...] = residual
    for b in range(blocks_ref.shape[0]):
        blocks_ref[b] = residual


def pack_kernel(gate_ref, up_ref, down_ref, out_ref):
    units, width = gate_ref.shape
    for n, ref in enumerate((gate_ref, up_ref, down_ref)):
        out_ref[n, 0:units, :] = ref[...]
        out_ref[n, units:, :] = jnp.zeros((UNITS - units, width), BF16)


def feed_forward_kernel(
    side, tiles_ref, gain_ref, own_ref, above_ref, below_ref, far_low_ref, far_high_ref,
    out_ref, xn_ref,
):
    peers, count, part = tiles_ref.shape
    tp = peers // side
    half = far_low_ref.shape[2]
    for x in range(side):
        norm_rows(tiles_ref, x * tp, tp, gain_ref, xn_ref, x * count)
    xn = xn_ref[...]

    def pre_of(ref, cols):
        block = ref[0:2].reshape(2 * UNITS, ref.shape[2])
        return lax.dot_general(xn[:, cols], block, NT, preferred_element_type=F32)

    every = slice(None)
    pres = [pre_of(ref, every) for ref in (own_ref, above_ref, below_ref)]
    pres.append(
        pre_of(far_low_ref, slice(0, half)) + pre_of(far_high_ref, slice(half, 2 * half))
    )
    hidden = [(silu(pre[:, :UNITS]) * pre[:, UNITS:]).astype(BF16) for pre in pres]
    for t in range(tp):
        cols = slice(t * part, (t + 1) * part)
        if (t + 1) * part <= half:
            far = far_low_ref[2, :, cols]
        else:
            far = far_high_ref[2, :, slice(t * part - half, (t + 1) * part - half)]
        parts = (own_ref[2, :, cols], above_ref[2, :, cols], below_ref[2, :, cols], far)
        down = jnp.dot(hidden[0], parts[0], preferred_element_type=F32)
        for n in range(1, len(parts)):
            down = down + jnp.dot(hidden[n], parts[n], preferred_element_type=F32)
        down = down.astype(BF16)
        for x in range(side):
            out_ref[x * tp + t] = down[x * count : (x + 1) * count]


def body(
    tokens,
    attn_gain,
    w_query,
    w_key,
    w_value,
    w_outgate,
    w_rates,
    head_rate,
    head_gain,
    w_out,
    state,
    mlp_gain,
    w_gate,
    w_up,
    w_down,
):
    count, part = tokens.shape
    tp = lax.axis_size("tp")
    side = 4
    width = part * tp
    size = w_query.shape[1]
    peers = side * tp
    groups = plane_groups(side, tp)

    own = pl.pallas_call(
        pack_kernel,
        out_shape=pltpu.VMEM((3, UNITS, width), BF16),
        in_specs=[VMEM] * 3,
        out_specs=VMEM,
        compiler_params=pltpu.CompilerParams(vmem_limit_bytes=4 << 20),
        name="pack",
    )(w_gate.T, w_up.T, w_down.T)
    above = lax.ppermute(own, "kv", y_ring(1, side))
    below = lax.ppermute(own, "kv", y_ring(-1, side))
    copies = jnp.broadcast_to(tokens[None], (tp, count, part))
    copies, own = lax.optimization_barrier((copies, own))
    tiles = lax.all_to_all(copies, "tp", 0, 0, tiled=True)
    tiles, new_state = pl.pallas_call(
        attention_kernel,
        out_shape=(
            pltpu.VMEM((tp, count, part), BF16),
            jax.ShapeDtypeStruct((count, size, size), F32),
        ),
        in_specs=[VMEM] * 11,
        out_specs=(VMEM, VMEM),
        scratch_shapes=[
            pltpu.VMEM((count, width), BF16),
            pltpu.VMEM((count, size), F32),
            pltpu.VMEM((count, size), F32),
        ],
        compiler_params=pltpu.CompilerParams(vmem_limit_bytes=16 << 20),
        name="attention",
    )(
        tiles,
        attn_gain.reshape(1, width),
        w_query,
        w_key,
        w_value,
        w_outgate,
        w_rates.reshape(2, width),
        head_rate.reshape(1, 1),
        head_gain.reshape(1, size),
        w_out,
        state.reshape(count, size, size),
    )
    tiles = lax.all_to_all(tiles, "tp", 0, 0, tiled=True)
    residual, blocks = pl.pallas_call(
        residual_kernel,
        out_shape=(
            pltpu.VMEM((count, part), BF16),
            pltpu.VMEM((peers, count, part), BF16),
        ),
        in_specs=[VMEM, VMEM],
        out_specs=(VMEM, VMEM),
        compiler_params=pltpu.CompilerParams(vmem_limit_bytes=4 << 20),
        name="residual",
    )(tiles, tokens)

    blocks, above, below = lax.optimization_barrier((blocks, above, below))
    far_low = lax.ppermute(above[:, :, : width // 2], "kv", y_ring(1, side))
    far_high = lax.ppermute(below[:, :, width // 2 :], "kv", y_ring(-1, side))
    tiles = lax.all_to_all(
        blocks, ("kv", "tp"), 0, 0, tiled=True, axis_index_groups=groups
    )
    tiles = pl.pallas_call(
        functools.partial(feed_forward_kernel, side),
        out_shape=pltpu.VMEM((peers, count, part), BF16),
        in_specs=[VMEM] * 7,
        out_specs=VMEM,
        scratch_shapes=[pltpu.VMEM((side * count, width), BF16)],
        compiler_params=pltpu.CompilerParams(vmem_limit_bytes=16 << 20),
        name="feed_forward",
    )(tiles, mlp_gain.reshape(1, width), *in_vmem(own, above, below, far_low, far_high))
    tiles = lax.all_to_all(
        tiles, ("kv", "tp"), 0, 0, tiled=True, axis_index_groups=groups
    )
    down = jnp.sum(tiles.astype(F32), axis=0)
    result = (residual.astype(F32) + down).astype(BF16)
    return (result, new_state[:, None])


def solution(mesh):
    return jax.shard_map(
        body,
        mesh=mesh,
        in_specs=(
            P("kv", "tp"),
            P(),
            P(None, "tp"),
            P(None, "tp"),
            P(None, "tp"),
            P(None, "tp"),
            P(None, None, "tp"),
            P("tp"),
            P("tp"),
            P("tp", None),
            P("kv", "tp", None, None),
            P(),
            P(None, ("kv", "tp")),
            P(None, ("kv", "tp")),
            P(None, ("kv", "tp")),
        ),
        out_specs=(P("kv", "tp"), P("kv", "tp", None, None)),
        check_vma=False,
    )
```

```python
import functools

import jax
import jax.numpy as jnp
from jax import lax
from jax.experimental import pallas as pl
from jax.experimental.pallas import tpu as pltpu
from jax.sharding import PartitionSpec as P


EPS = 1e-06
UNITS = 48
F32, BF16 = jnp.float32, jnp.bfloat16
NT = (((1,), (1,)), ((), ()))
VMEM = pl.BlockSpec(memory_space=pltpu.VMEM)
SMEM = pl.BlockSpec(memory_space=pltpu.SMEM)
HBM = pl.BlockSpec(memory_space=pltpu.HBM)


def in_hbm(*arrays):
    return [pltpu.with_memory_space_constraint(a, pltpu.HBM) for a in arrays]


def in_vmem(*arrays):
    return [pltpu.with_memory_space_constraint(a, pltpu.VMEM) for a in arrays]


def y_ring(shift, side):
    return [
        (side * y + x, side * ((y + shift) % side) + x) for y in range(side) for x in range(side)
    ]


def plane_groups(side, tp):
    return [[(side * y + x) * tp + t for x in range(side) for t in range(tp)] for y in range(side)]


def silu(t):
    return t / (1.0 + jnp.exp(-t))


def norm_rows(tiles_ref, first, n_tiles, gain_ref, out_ref, at):
    rows, part = tiles_ref.shape[1:]
    total = jnp.zeros((rows, part), F32)
    for t in range(n_tiles):
        tile = tiles_ref[first + t].astype(F32)
        total = total + tile * tile
    mean = jnp.sum(total, axis=-1, keepdims=True) * (1.0 / (n_tiles * part))
    scale = lax.rsqrt(mean + EPS)
    for t in range(n_tiles):
        cols = slice(t * part, (t + 1) * part)
        tile = tiles_ref[first + t].astype(F32)
        out_ref[at : at + rows, cols] = (tile * scale * gain_ref[0:1, cols]).astype(BF16)


def attention_kernel(
    tiles_ref, gain_ref, wr_ref, rate_ref, head_gain_ref, wq_hbm, wk_hbm, wv_hbm, wg_hbm, wo_hbm,
    state_hbm, out_ref, new_state_hbm, xn_ref, u_ref, w_ref, wq_ref, wk_ref, wv_ref, wg_ref,
    wo_ref, state_ref, new_state_ref, sems, out_sems,
):
    tp, count, part = tiles_ref.shape
    size = wq_ref.shape[1]
    loads = [
        pltpu.make_async_copy(source, target, sems.at[n])
        for n, (source, target) in enumerate(
            (
                (wq_hbm, wq_ref),
                (wk_hbm, wk_ref),
                (state_hbm, state_ref),
                (wv_hbm, wv_ref),
                (wg_hbm, wg_ref),
                (wo_hbm, wo_ref),
            )
        )
    ]
    for load in loads:
        load.start()
    norm_rows(tiles_ref, 0, tp, gain_ref, xn_ref, 0)
    xn = xn_ref[...]
    rates = lax.dot_general(xn, wr_ref[...], NT, preferred_element_type=F32)
    loads[0].wait()
    query = jnp.dot(xn, wq_ref[...], preferred_element_type=F32)
    loads[1].wait()
    key = jnp.dot(xn, wk_ref[...], preferred_element_type=F32)
    strength = 1.0 / (1.0 + jnp.exp(-rates[:, 0:1]))
    decay = rates[:, 1:2]
    softplus = jnp.maximum(decay, 0.0) + jnp.log(1.0 + jnp.exp(-jnp.abs(decay)))
    fade = jnp.exp(-rate_ref[...] * softplus)
    q = query * lax.rsqrt(jnp.sum(query * query, -1, keepdims=True) + EPS) * size**-0.5
    k = key * lax.rsqrt(jnp.sum(key * key, -1, keepdims=True) + EPS)
    q_high, k_high = q.astype(BF16), k.astype(BF16)
    q_low = (q - q_high.astype(F32)).astype(BF16)
    k_low = (k - k_high.astype(F32)).astype(BF16)
    probes = jnp.concatenate([k_high, k_low, q_high, q_low], axis=0)
    loads[2].wait()
    for b in range(count):
        read = jnp.dot(probes, state_ref[b].astype(BF16), preferred_element_type=F32)
        u_ref[b : b + 1, :] = read[b : b + 1] + read[count + b : count + b + 1]
        w_ref[b : b + 1, :] = read[2 * count + b : 2 * count + b + 1] + read[
            3 * count + b : 3 * count + b + 1
        ]
    loads[3].wait()
    value = jnp.dot(xn, wv_ref[...], preferred_element_type=F32)
    loads[4].wait()
    gate_in = jnp.dot(xn, wg_ref[...], preferred_element_type=F32)
    fresh = strength * (value - fade * u_ref[...])
    readout = fade * w_ref[...] + jnp.sum(q * k, -1, keepdims=True) * fresh
    k_columns = k.T
    stores = []
    for b in range(count):
        new_state_ref[b] = (
            fade[b : b + 1, :] * state_ref[b] + k_columns[:, b : b + 1] * fresh[b : b + 1, :]
        )
        if b % 4 == 3:
            rows = pl.ds(b - 3, 4)
            stores.append(
                pltpu.make_async_copy(
                    new_state_ref.at[rows], new_state_hbm.at[rows], out_sems.at[b // 4]
                )
            )
            stores[-1].start()
    scale = lax.rsqrt(jnp.mean(readout * readout, -1, keepdims=True) + EPS)
    mixed = (readout * scale * head_gain_ref[...] * silu(gate_in)).astype(BF16)
    loads[5].wait()
    for t in range(tp):
        cols = slice(t * part, (t + 1) * part)
        out_ref[t] = jnp.dot(mixed, wo_ref[:, cols], preferred_element_type=F32).astype(BF16)
    for store in stores:
        store.wait()


def residual_kernel(tiles_ref, tokens_ref, out_ref, blocks_ref):
    total = tokens_ref[...].astype(F32)
    for t in range(tiles_ref.shape[0]):
        total = total + tiles_ref[t].astype(F32)
    residual = total.astype(BF16)
    out_ref[...] = residual
    for b in range(blocks_ref.shape[0]):
        blocks_ref[b] = residual


def pack_kernel(
    rate_ref, gate_ref, up_ref, down_ref, tokens_ref, own_ref, copies_ref, rate_row_ref,
    gate_at, up_at, down_at, sems,
):
    units = gate_ref.shape[0]
    landed = (gate_at, up_at, down_at)
    moves = [
        pltpu.make_async_copy(ref, at, sems.at[n])
        for n, (ref, at) in enumerate(zip((gate_ref, up_ref, down_ref), landed))
    ]
    for move in moves:
        move.start()
    for b in range(copies_ref.shape[0]):
        copies_ref[b] = tokens_ref[...]
    rate_row_ref[...] = jnp.full(rate_row_ref.shape, rate_ref[0], F32)
    for n, (move, at) in enumerate(zip(moves, landed)):
        move.wait()
        own_ref[n, 0:units, :] = at[...]
        own_ref[n, units:, :] = jnp.zeros((UNITS - units, own_ref.shape[2]), BF16)


def pre_of(xn, ref):
    block = ref[0:2].reshape(2 * UNITS, ref.shape[2])
    return lax.dot_general(xn, block, NT, preferred_element_type=F32)


def hidden_of(pre):
    return (silu(pre[:, :UNITS]) * pre[:, UNITS:]).astype(BF16)


def near_kernel(side, tiles_ref, gain_ref, own_ref, above_ref, below_ref, xn_ref, hidden_ref):
    peers, count, _ = tiles_ref.shape
    tp = peers // side
    for x in range(side):
        norm_rows(tiles_ref, x * tp, tp, gain_ref, xn_ref, x * count)
    xn = xn_ref[...]
    for n, ref in enumerate((own_ref, above_ref, below_ref)):
        hidden_ref[n] = hidden_of(pre_of(xn, ref))


def far_kernel(
    side, xn_ref, hidden_ref, own_ref, above_ref, below_ref, far_low_ref, far_high_ref, out_ref
):
    peers, count, part = out_ref.shape
    tp = peers // side
    half = far_low_ref.shape[2]
    pre = pre_of(xn_ref[:, :half], far_low_ref) + pre_of(xn_ref[:, half:], far_high_ref)
    hidden = [hidden_ref[n] for n in range(3)] + [hidden_of(pre)]
    for t in range(tp):
        cols = slice(t * part, (t + 1) * part)
        if (t + 1) * part <= half:
            far = far_low_ref[2, :, cols]
        else:
            far = far_high_ref[2, :, slice(t * part - half, (t + 1) * part - half)]
        parts = (own_ref[2, :, cols], above_ref[2, :, cols], below_ref[2, :, cols], far)
        down = jnp.dot(hidden[0], parts[0], preferred_element_type=F32)
        for n in range(1, len(parts)):
            down = down + jnp.dot(hidden[n], parts[n], preferred_element_type=F32)
        down = down.astype(BF16)
        for x in range(side):
            out_ref[x * tp + t] = down[x * count : (x + 1) * count]


def body(
    tokens,
    attn_gain,
    w_query,
    w_key,
    w_value,
    w_outgate,
    w_rates,
    head_rate,
    head_gain,
    w_out,
    state,
    mlp_gain,
    w_gate,
    w_up,
    w_down,
):
    count, part = tokens.shape
    tp = lax.axis_size("tp")
    side = 4
    width = part * tp
    size = w_query.shape[1]
    peers = side * tp
    groups = plane_groups(side, tp)

    own, copies, rate_row = pl.pallas_call(
        pack_kernel,
        out_shape=(
            pltpu.VMEM((3, UNITS, width), BF16),
            pltpu.VMEM((tp, count, part), BF16),
            pltpu.VMEM((1, size), F32),
        ),
        in_specs=[SMEM] + [HBM] * 3 + [VMEM],
        out_specs=(VMEM, VMEM, VMEM),
        scratch_shapes=[pltpu.VMEM((w_gate.shape[1], width), BF16)] * 3
        + [pltpu.SemaphoreType.DMA((3,))],
        compiler_params=pltpu.CompilerParams(vmem_limit_bytes=4 << 20),
        name="pack",
    )(head_rate, *in_hbm(w_gate.T, w_up.T, w_down.T), tokens)
    above = lax.ppermute(own, "kv", y_ring(1, side))
    below = lax.ppermute(own, "kv", y_ring(-1, side))
    tiles = lax.all_to_all(copies, "tp", 0, 0, tiled=True)
    weight = pltpu.VMEM((width, size), BF16)
    states = pltpu.VMEM((count, size, size), F32)
    tiles, new_state = pl.pallas_call(
        attention_kernel,
        out_shape=(
            pltpu.VMEM((tp, count, part), BF16),
            pltpu.HBM((count, size, size), F32),
        ),
        in_specs=[VMEM] * 5 + [HBM] * 6,
        out_specs=(VMEM, HBM),
        scratch_shapes=[
            pltpu.VMEM((count, width), BF16),
            pltpu.VMEM((count, size), F32),
            pltpu.VMEM((count, size), F32),
            weight,
            weight,
            weight,
            weight,
            pltpu.VMEM((size, width), BF16),
            states,
            states,
            pltpu.SemaphoreType.DMA((6,)),
            pltpu.SemaphoreType.DMA((4,)),
        ],
        compiler_params=pltpu.CompilerParams(vmem_limit_bytes=16 << 20),
        name="attention",
    )(
        tiles,
        attn_gain.reshape(1, width),
        w_rates.reshape(2, width),
        rate_row,
        head_gain.reshape(1, size),
        *in_hbm(
            w_query, w_key, w_value, w_outgate, w_out, state.reshape(count, size, size)
        ),
    )
    tiles = lax.all_to_all(tiles, "tp", 0, 0, tiled=True)
    residual, blocks = pl.pallas_call(
        residual_kernel,
        out_shape=(
            pltpu.VMEM((count, part), BF16),
            pltpu.VMEM((peers, count, part), BF16),
        ),
        in_specs=[VMEM, VMEM],
        out_specs=(VMEM, VMEM),
        compiler_params=pltpu.CompilerParams(vmem_limit_bytes=4 << 20),
        name="residual",
    )(tiles, tokens)

    blocks, above, below = lax.optimization_barrier((blocks, above, below))
    far_low = lax.ppermute(above[:, :, : width // 2], "kv", y_ring(1, side))
    far_high = lax.ppermute(below[:, :, width // 2 :], "kv", y_ring(-1, side))
    tiles = lax.all_to_all(
        blocks, ("kv", "tp"), 0, 0, tiled=True, axis_index_groups=groups
    )
    xn, hidden = pl.pallas_call(
        functools.partial(near_kernel, side),
        out_shape=(
            pltpu.VMEM((side * count, width), BF16),
            pltpu.VMEM((3, side * count, UNITS), BF16),
        ),
        in_specs=[VMEM] * 5,
        out_specs=(VMEM, VMEM),
        compiler_params=pltpu.CompilerParams(vmem_limit_bytes=16 << 20),
        name="near",
    )(tiles, mlp_gain.reshape(1, width), *in_vmem(own, above, below))
    tiles = pl.pallas_call(
        functools.partial(far_kernel, side),
        out_shape=pltpu.VMEM((peers, count, part), BF16),
        in_specs=[VMEM] * 7,
        out_specs=VMEM,
        compiler_params=pltpu.CompilerParams(vmem_limit_bytes=16 << 20),
        name="far",
    )(xn, hidden, *in_vmem(own, above, below, far_low, far_high))
    tiles = lax.all_to_all(
        tiles, ("kv", "tp"), 0, 0, tiled=True, axis_index_groups=groups
    )
    down = jnp.sum(tiles.astype(F32), axis=0)
    result = (residual.astype(F32) + down).astype(BF16)
    return (result, new_state[:, None])


def solution(mesh):
    return jax.shard_map(
        body,
        mesh=mesh,
        in_specs=(
            P("kv", "tp"),
            P(),
            P(None, "tp"),
            P(None, "tp"),
            P(None, "tp"),
            P(None, "tp"),
            P(None, None, "tp"),
            P("tp"),
            P("tp"),
            P("tp", None),
            P("kv", "tp", None, None),
            P(),
            P(None, ("kv", "tp")),
            P(None, ("kv", "tp")),
            P(None, ("kv", "tp")),
        ),
        out_specs=(P("kv", "tp"), P("kv", "tp", None, None)),
        check_vma=False,
    )
```

```python
import functools

import jax
import jax.numpy as jnp
from jax import lax
from jax.experimental import pallas as pl
from jax.experimental.pallas import tpu as pltpu
from jax.sharding import PartitionSpec as P


EPS = 1e-06
UNITS = 48
F32, BF16 = jnp.float32, jnp.bfloat16
NT = (((1,), (1,)), ((), ()))
VMEM = pl.BlockSpec(memory_space=pltpu.VMEM)
SMEM = pl.BlockSpec(memory_space=pltpu.SMEM)
HBM = pl.BlockSpec(memory_space=pltpu.HBM)


def in_hbm(*arrays):
    return [pltpu.with_memory_space_constraint(a, pltpu.HBM) for a in arrays]


def in_vmem(*arrays):
    return [pltpu.with_memory_space_constraint(a, pltpu.VMEM) for a in arrays]


def y_ring(shift, side):
    return [
        (side * y + x, side * ((y + shift) % side) + x) for y in range(side) for x in range(side)
    ]


def plane_groups(side, tp):
    return [[(side * y + x) * tp + t for x in range(side) for t in range(tp)] for y in range(side)]


def silu(t):
    return t / (1.0 + jnp.exp(-t))


def norm_rows(tiles_ref, first, n_tiles, gain_ref, out_ref, at):
    rows, part = tiles_ref.shape[1:]
    total = jnp.zeros((rows, part), F32)
    for t in range(n_tiles):
        tile = tiles_ref[first + t].astype(F32)
        total = total + tile * tile
    mean = jnp.sum(total, axis=-1, keepdims=True) * (1.0 / (n_tiles * part))
    scale = lax.rsqrt(mean + EPS)
    for t in range(n_tiles):
        cols = slice(t * part, (t + 1) * part)
        tile = tiles_ref[first + t].astype(F32)
        out_ref[at : at + rows, cols] = (tile * scale * gain_ref[0:1, cols]).astype(BF16)


def attention_kernel(
    tiles_ref, gain_ref, wr_ref, rate_ref, head_gain_ref, wq_hbm, wk_hbm, wv_hbm, wg_hbm, wo_hbm,
    state_hbm, out_ref, new_state_hbm, xn_ref, u_ref, w_ref, wq_ref, wk_ref, wv_ref, wg_ref,
    wo_ref, state_ref, new_state_ref, sems, out_sems,
):
    tp, count, part = tiles_ref.shape
    size = wq_ref.shape[1]
    loads = [
        pltpu.make_async_copy(source, target, sems.at[n])
        for n, (source, target) in enumerate(
            (
                (wq_hbm, wq_ref),
                (wk_hbm, wk_ref),
                (state_hbm, state_ref),
                (wv_hbm, wv_ref),
                (wg_hbm, wg_ref),
                (wo_hbm, wo_ref),
            )
        )
    ]
    for load in loads:
        load.start()
    norm_rows(tiles_ref, 0, tp, gain_ref, xn_ref, 0)
    xn = xn_ref[...]
    rates = lax.dot_general(xn, wr_ref[...], NT, preferred_element_type=F32)
    loads[0].wait()
    query = jnp.dot(xn, wq_ref[...], preferred_element_type=F32)
    loads[1].wait()
    key = jnp.dot(xn, wk_ref[...], preferred_element_type=F32)
    strength = 1.0 / (1.0 + jnp.exp(-rates[:, 0:1]))
    decay = rates[:, 1:2]
    softplus = jnp.maximum(decay, 0.0) + jnp.log(1.0 + jnp.exp(-jnp.abs(decay)))
    fade = jnp.exp(-rate_ref[...] * softplus)
    q = query * lax.rsqrt(jnp.sum(query * query, -1, keepdims=True) + EPS) * size**-0.5
    k = key * lax.rsqrt(jnp.sum(key * key, -1, keepdims=True) + EPS)
    q_high, k_high = q.astype(BF16), k.astype(BF16)
    q_low = (q - q_high.astype(F32)).astype(BF16)
    k_low = (k - k_high.astype(F32)).astype(BF16)
    probes = jnp.concatenate([k_high, k_low, q_high, q_low], axis=0)
    loads[2].wait()
    for b in range(count):
        read = jnp.dot(probes, state_ref[b].astype(BF16), preferred_element_type=F32)
        u_ref[b : b + 1, :] = read[b : b + 1] + read[count + b : count + b + 1]
        w_ref[b : b + 1, :] = read[2 * count + b : 2 * count + b + 1] + read[
            3 * count + b : 3 * count + b + 1
        ]
    loads[3].wait()
    value = jnp.dot(xn, wv_ref[...], preferred_element_type=F32)
    loads[4].wait()
    gate_in = jnp.dot(xn, wg_ref[...], preferred_element_type=F32)
    fresh = strength * (value - fade * u_ref[...])
    readout = fade * w_ref[...] + jnp.sum(q * k, -1, keepdims=True) * fresh
    k_columns = k.T
    stores = []
    for b in range(count):
        new_state_ref[b] = (
            fade[b : b + 1, :] * state_ref[b] + k_columns[:, b : b + 1] * fresh[b : b + 1, :]
        )
        if b % 4 == 3:
            rows = pl.ds(b - 3, 4)
            stores.append(
                pltpu.make_async_copy(
                    new_state_ref.at[rows], new_state_hbm.at[rows], out_sems.at[b // 4]
                )
            )
            stores[-1].start()
    scale = lax.rsqrt(jnp.mean(readout * readout, -1, keepdims=True) + EPS)
    mixed = (readout * scale * head_gain_ref[...] * silu(gate_in)).astype(BF16)
    loads[5].wait()
    for t in range(tp):
        cols = slice(t * part, (t + 1) * part)
        out_ref[t] = jnp.dot(mixed, wo_ref[:, cols], preferred_element_type=F32).astype(BF16)
    for store in stores:
        store.wait()


def residual_kernel(tiles_ref, tokens_ref, out_ref, blocks_ref):
    total = tokens_ref[...].astype(F32)
    for t in range(tiles_ref.shape[0]):
        total = total + tiles_ref[t].astype(F32)
    residual = total.astype(BF16)
    out_ref[...] = residual
    rows = blocks_ref.shape[1]
    for b in range(blocks_ref.shape[0]):
        at = (b % 2) * rows
        blocks_ref[b] = residual[at : at + rows]


def pack_kernel(
    rate_ref, gate_ref, up_ref, down_ref, tokens_ref, own_ref, copies_ref, rate_row_ref,
    gate_at, up_at, down_at, sems,
):
    units = gate_ref.shape[0]
    landed = (gate_at, up_at, down_at)
    moves = [
        pltpu.make_async_copy(ref, at, sems.at[n])
        for n, (ref, at) in enumerate(zip((gate_ref, up_ref, down_ref), landed))
    ]
    for move in moves:
        move.start()
    for b in range(copies_ref.shape[0]):
        copies_ref[b] = tokens_ref[...]
    rate_row_ref[...] = jnp.full(rate_row_ref.shape, rate_ref[0], F32)
    for n, (move, at) in enumerate(zip(moves, landed)):
        move.wait()
        own_ref[n, 0:units, :] = at[...]
        own_ref[n, units:, :] = jnp.zeros((UNITS - units, own_ref.shape[2]), BF16)


def pre_of(xn, ref):
    block = ref[0:2].reshape(2 * UNITS, ref.shape[2])
    return lax.dot_general(xn, block, NT, preferred_element_type=F32)


def hidden_of(pre):
    return (silu(pre[:, :UNITS]) * pre[:, UNITS:]).astype(BF16)


def norm_kernel(side, tiles_ref, gain_ref, xn_ref):
    peers, count, _ = tiles_ref.shape
    tp = peers // side
    for x in range(side):
        norm_rows(tiles_ref, x * tp, tp, gain_ref, xn_ref, x * count)


def far_parts(far_low_ref, far_high_ref, part):
    half = far_low_ref.shape[2]

    def pre(xn_ref):
        return pre_of(xn_ref[:, :half], far_low_ref) + pre_of(xn_ref[:, half:], far_high_ref)

    def columns(t):
        if (t + 1) * part <= half:
            return far_low_ref[2, :, t * part : (t + 1) * part]
        return far_high_ref[2, :, t * part - half : (t + 1) * part - half]

    return pre, columns


def near_kernel(part, xn_ref, *refs):
    *whole, far_low_ref, far_high_ref, out_ref = refs
    far_pre, far_columns = far_parts(far_low_ref, far_high_ref, part)
    xn = xn_ref[...]
    hidden = [hidden_of(pre_of(xn, ref)) for ref in whole]
    hidden.append(hidden_of(far_pre(xn_ref)))
    for t in range(out_ref.shape[1] // part):
        cols = slice(t * part, (t + 1) * part)
        down = jnp.dot(hidden[-1], far_columns(t), preferred_element_type=F32)
        for n, ref in enumerate(whole):
            down = down + jnp.dot(hidden[n], ref[2, :, cols], preferred_element_type=F32)
        out_ref[:, cols] = down


def far_kernel(side, xn_ref, near_ref, far_low_ref, far_high_ref, out_ref):
    peers, count, part = out_ref.shape
    tp = peers // side
    far_pre, far_columns = far_parts(far_low_ref, far_high_ref, part)
    hidden = hidden_of(far_pre(xn_ref))
    for t in range(tp):
        cols = slice(t * part, (t + 1) * part)
        down = near_ref[:, cols] + jnp.dot(hidden, far_columns(t), preferred_element_type=F32)
        down = down.astype(BF16)
        for x in range(side):
            out_ref[x * tp + t] = down[x * count : (x + 1) * count]


def body(
    tokens,
    attn_gain,
    w_query,
    w_key,
    w_value,
    w_outgate,
    w_rates,
    head_rate,
    head_gain,
    w_out,
    state,
    mlp_gain,
    w_gate,
    w_up,
    w_down,
):
    count, part = tokens.shape
    tp = lax.axis_size("tp")
    side = 4
    width = part * tp
    size = w_query.shape[1]
    peers = side * tp
    groups = plane_groups(side, tp)

    own, copies, rate_row = pl.pallas_call(
        pack_kernel,
        out_shape=(
            pltpu.VMEM((3, UNITS, width), BF16),
            pltpu.VMEM((tp, count, part), BF16),
            pltpu.VMEM((1, size), F32),
        ),
        in_specs=[SMEM] + [HBM] * 3 + [VMEM],
        out_specs=(VMEM, VMEM, VMEM),
        scratch_shapes=[pltpu.VMEM((w_gate.shape[1], width), BF16)] * 3
        + [pltpu.SemaphoreType.DMA((3,))],
        compiler_params=pltpu.CompilerParams(vmem_limit_bytes=4 << 20),
        name="pack",
    )(head_rate, *in_hbm(w_gate.T, w_up.T, w_down.T), tokens)
    above = lax.ppermute(own, "kv", y_ring(1, side))
    below = lax.ppermute(own, "kv", y_ring(-1, side))
    tiles = lax.all_to_all(copies, "tp", 0, 0, tiled=True)
    weight = pltpu.VMEM((width, size), BF16)
    states = pltpu.VMEM((count, size, size), F32)
    tiles, new_state = pl.pallas_call(
        attention_kernel,
        out_shape=(
            pltpu.VMEM((tp, count, part), BF16),
            pltpu.HBM((count, size, size), F32),
        ),
        in_specs=[VMEM] * 5 + [HBM] * 6,
        out_specs=(VMEM, HBM),
        scratch_shapes=[
            pltpu.VMEM((count, width), BF16),
            pltpu.VMEM((count, size), F32),
            pltpu.VMEM((count, size), F32),
            weight,
            weight,
            weight,
            weight,
            pltpu.VMEM((size, width), BF16),
            states,
            states,
            pltpu.SemaphoreType.DMA((6,)),
            pltpu.SemaphoreType.DMA((4,)),
        ],
        compiler_params=pltpu.CompilerParams(vmem_limit_bytes=16 << 20),
        name="attention",
    )(
        tiles,
        attn_gain.reshape(1, width),
        w_rates.reshape(2, width),
        rate_row,
        head_gain.reshape(1, size),
        *in_hbm(
            w_query, w_key, w_value, w_outgate, w_out, state.reshape(count, size, size)
        ),
    )
    tiles = lax.all_to_all(tiles, "tp", 0, 0, tiled=True)
    half_count = count // 2
    residual, blocks = pl.pallas_call(
        residual_kernel,
        out_shape=(
            pltpu.VMEM((count, part), BF16),
            pltpu.VMEM((peers, half_count, part), BF16),
        ),
        in_specs=[VMEM, VMEM],
        out_specs=(VMEM, VMEM),
        compiler_params=pltpu.CompilerParams(vmem_limit_bytes=4 << 20),
        name="residual",
    )(tiles, tokens)

    blocks, own, above, below = lax.optimization_barrier((blocks, own, above, below))
    far_low = lax.ppermute(above[:, :, : width // 2], "kv", y_ring(1, side))
    far_high = lax.ppermute(below[:, :, width // 2 :], "kv", y_ring(-1, side))
    partner = [(t, t ^ 1) for t in range(tp)]
    own_2 = lax.ppermute(own, "tp", partner)
    above_2 = lax.ppermute(above, "tp", partner)
    below_2 = lax.ppermute(below, "tp", partner)
    tiles = lax.all_to_all(
        blocks, ("kv", "tp"), 0, 0, tiled=True, axis_index_groups=groups
    )
    rows = side * half_count
    xn = pl.pallas_call(
        functools.partial(norm_kernel, side),
        out_shape=pltpu.VMEM((rows, width), BF16),
        in_specs=[VMEM] * 2,
        out_specs=VMEM,
        compiler_params=pltpu.CompilerParams(vmem_limit_bytes=4 << 20),
        name="norm",
    )(tiles, mlp_gain.reshape(1, width))
    xn, far_low, far_high = lax.optimization_barrier((xn, far_low, far_high))
    far_low_2 = lax.ppermute(far_low, "tp", partner)
    far_high_2 = lax.ppermute(far_high, "tp", partner)
    near = pl.pallas_call(
        functools.partial(near_kernel, part),
        out_shape=pltpu.VMEM((rows, width), F32),
        in_specs=[VMEM] * 9,
        out_specs=VMEM,
        compiler_params=pltpu.CompilerParams(vmem_limit_bytes=8 << 20),
        cost_estimate=pl.CostEstimate(
            flops=8_000_000_000, bytes_accessed=8_000_000, transcendentals=0
        ),
        name="near",
    )(xn, *in_vmem(own, above, below, own_2, above_2, below_2, far_low, far_high))
    tiles = pl.pallas_call(
        functools.partial(far_kernel, side),
        out_shape=pltpu.VMEM((peers, half_count, part), BF16),
        in_specs=[VMEM] * 4,
        out_specs=VMEM,
        compiler_params=pltpu.CompilerParams(vmem_limit_bytes=8 << 20),
        name="far",
    )(xn, near, *in_vmem(far_low_2, far_high_2))
    tiles = lax.all_to_all(
        tiles, ("kv", "tp"), 0, 0, tiled=True, axis_index_groups=groups
    )
    tiles = tiles.astype(F32).reshape(peers // 2, count, part)
    result = (residual.astype(F32) + jnp.sum(tiles, axis=0)).astype(BF16)
    return (result, new_state[:, None])


def solution(mesh):
    return jax.shard_map(
        body,
        mesh=mesh,
        in_specs=(
            P("kv", "tp"),
            P(),
            P(None, "tp"),
            P(None, "tp"),
            P(None, "tp"),
            P(None, "tp"),
            P(None, None, "tp"),
            P("tp"),
            P("tp"),
            P("tp", None),
            P("kv", "tp", None, None),
            P(),
            P(None, ("kv", "tp")),
            P(None, ("kv", "tp")),
            P(None, ("kv", "tp")),
        ),
        out_specs=(P("kv", "tp"), P("kv", "tp", None, None)),
        check_vma=False,
    )
```

```python
import functools

import jax
import jax.numpy as jnp
from jax import lax
from jax.experimental import pallas as pl
from jax.experimental.pallas import tpu as pltpu
from jax.sharding import PartitionSpec as P


EPS = 1e-06
UNITS = 48
F32, BF16 = jnp.float32, jnp.bfloat16
NT = (((1,), (1,)), ((), ()))
VMEM = pl.BlockSpec(memory_space=pltpu.VMEM)
SMEM = pl.BlockSpec(memory_space=pltpu.SMEM)
HBM = pl.BlockSpec(memory_space=pltpu.HBM)


def in_hbm(*arrays):
    return [pltpu.with_memory_space_constraint(a, pltpu.HBM) for a in arrays]


def in_vmem(*arrays):
    return [pltpu.with_memory_space_constraint(a, pltpu.VMEM) for a in arrays]


def y_ring(shift, side):
    return [
        (side * y + x, side * ((y + shift) % side) + x) for y in range(side) for x in range(side)
    ]


def plane_groups(side, tp):
    return [[(side * y + x) * tp + t for x in range(side) for t in range(tp)] for y in range(side)]


def silu(t):
    return t / (1.0 + jnp.exp(-t))


def norm_rows(tiles_ref, first, n_tiles, gain_ref, out_ref, at):
    rows, part = tiles_ref.shape[1:]
    total = jnp.zeros((rows, part), F32)
    for t in range(n_tiles):
        tile = tiles_ref[first + t].astype(F32)
        total = total + tile * tile
    mean = jnp.sum(total, axis=-1, keepdims=True) * (1.0 / (n_tiles * part))
    scale = lax.rsqrt(mean + EPS)
    for t in range(n_tiles):
        cols = slice(t * part, (t + 1) * part)
        tile = tiles_ref[first + t].astype(F32)
        out_ref[at : at + rows, cols] = (tile * scale * gain_ref[0:1, cols]).astype(BF16)


def attention_kernel(
    tiles_ref, gain_ref, wr_ref, rate_ref, head_gain_ref, wq_ref, wk_ref, wv_ref, wg_ref, wo_ref,
    state_ref, out_ref, new_state_hbm, xn_ref, u_ref, w_ref, new_state_ref, out_sems,
):
    tp, count, part = tiles_ref.shape
    size = wq_ref.shape[1]
    norm_rows(tiles_ref, 0, tp, gain_ref, xn_ref, 0)
    xn = xn_ref[...]
    rates = lax.dot_general(xn, wr_ref[...], NT, preferred_element_type=F32)
    query = jnp.dot(xn, wq_ref[...], preferred_element_type=F32)
    key = jnp.dot(xn, wk_ref[...], preferred_element_type=F32)
    strength = 1.0 / (1.0 + jnp.exp(-rates[:, 0:1]))
    decay = rates[:, 1:2]
    softplus = jnp.maximum(decay, 0.0) + jnp.log(1.0 + jnp.exp(-jnp.abs(decay)))
    fade = jnp.exp(-rate_ref[...] * softplus)
    q = query * lax.rsqrt(jnp.sum(query * query, -1, keepdims=True) + EPS) * size**-0.5
    k = key * lax.rsqrt(jnp.sum(key * key, -1, keepdims=True) + EPS)
    q_high, k_high = q.astype(BF16), k.astype(BF16)
    q_low = (q - q_high.astype(F32)).astype(BF16)
    k_low = (k - k_high.astype(F32)).astype(BF16)
    probes = jnp.concatenate([k_high, k_low, q_high, q_low], axis=0)
    for b in range(count):
        read = jnp.dot(probes, state_ref[b].astype(BF16), preferred_element_type=F32)
        u_ref[b : b + 1, :] = read[b : b + 1] + read[count + b : count + b + 1]
        w_ref[b : b + 1, :] = read[2 * count + b : 2 * count + b + 1] + read[
            3 * count + b : 3 * count + b + 1
        ]
    value = jnp.dot(xn, wv_ref[...], preferred_element_type=F32)
    gate_in = jnp.dot(xn, wg_ref[...], preferred_element_type=F32)
    fresh = strength * (value - fade * u_ref[...])
    readout = fade * w_ref[...] + jnp.sum(q * k, -1, keepdims=True) * fresh
    k_columns = k.T
    stores = []
    for b in range(count):
        new_state_ref[b] = (
            fade[b : b + 1, :] * state_ref[b] + k_columns[:, b : b + 1] * fresh[b : b + 1, :]
        )
        if b % 4 == 3:
            rows = pl.ds(b - 3, 4)
            stores.append(
                pltpu.make_async_copy(
                    new_state_ref.at[rows], new_state_hbm.at[rows], out_sems.at[b // 4]
                )
            )
            stores[-1].start()
    scale = lax.rsqrt(jnp.mean(readout * readout, -1, keepdims=True) + EPS)
    mixed = (readout * scale * head_gain_ref[...] * silu(gate_in)).astype(BF16)
    for t in range(tp):
        cols = slice(t * part, (t + 1) * part)
        out_ref[t] = jnp.dot(mixed, wo_ref[:, cols], preferred_element_type=F32).astype(BF16)
    for store in stores:
        store.wait()


def residual_kernel(tiles_ref, tokens_ref, out_ref, blocks_ref):
    total = tokens_ref[...].astype(F32)
    for t in range(tiles_ref.shape[0]):
        total = total + tiles_ref[t].astype(F32)
    residual = total.astype(BF16)
    out_ref[...] = residual
    rows = blocks_ref.shape[1]
    for b in range(blocks_ref.shape[0]):
        at = (b % 2) * rows
        blocks_ref[b] = residual[at : at + rows]


def pack_kernel(
    rate_ref, gate_hbm, up_hbm, down_hbm, tokens_hbm, own_ref, rate_row_ref, tokens_ref,
    gate_ref, up_ref, down_ref, sems,
):
    units = gate_ref.shape[0]
    landed = (tokens_ref, gate_ref, up_ref, down_ref)
    loads = [
        pltpu.make_async_copy(source, at, sems.at[n])
        for n, (source, at) in enumerate(
            zip((tokens_hbm, gate_hbm, up_hbm, down_hbm), landed)
        )
    ]
    for load in loads:
        load.start()
    for n in range(3):
        own_ref[n, units:, :] = jnp.zeros((UNITS - units, own_ref.shape[2]), BF16)
    rate_row_ref[...] = jnp.full(rate_row_ref.shape, rate_ref[0], F32)
    for n in range(3):
        loads[1 + n].wait()
        own_ref[n, 0:units, :] = landed[1 + n][...]
    loads[0].wait()


def spread_kernel(tokens_ref, copies_ref):
    for b in range(copies_ref.shape[0]):
        copies_ref[b] = tokens_ref[...]


def pre_of(xn, ref):
    block = ref[0:2].reshape(2 * UNITS, ref.shape[2])
    return lax.dot_general(xn, block, NT, preferred_element_type=F32)


def hidden_of(pre):
    return (silu(pre[:, :UNITS]) * pre[:, UNITS:]).astype(BF16)


def norm_kernel(side, tiles_ref, gain_ref, xn_ref):
    peers, count, _ = tiles_ref.shape
    tp = peers // side
    for x in range(side):
        norm_rows(tiles_ref, x * tp, tp, gain_ref, xn_ref, x * count)


def far_parts(far_low_ref, far_high_ref, part):
    half = far_low_ref.shape[2]

    def pre(xn_ref):
        return pre_of(xn_ref[:, :half], far_low_ref) + pre_of(xn_ref[:, half:], far_high_ref)

    def columns(t):
        if (t + 1) * part <= half:
            return far_low_ref[2, :, t * part : (t + 1) * part]
        return far_high_ref[2, :, t * part - half : (t + 1) * part - half]

    return pre, columns


def near_kernel(part, xn_ref, *refs):
    *whole, far_low_ref, far_high_ref, out_ref = refs
    far_pre, far_columns = far_parts(far_low_ref, far_high_ref, part)
    xn = xn_ref[...]
    hidden = [hidden_of(pre_of(xn, ref)) for ref in whole]
    hidden.append(hidden_of(far_pre(xn_ref)))
    for t in range(out_ref.shape[1] // part):
        cols = slice(t * part, (t + 1) * part)
        down = jnp.dot(hidden[-1], far_columns(t), preferred_element_type=F32)
        for n, ref in enumerate(whole):
            down = down + jnp.dot(hidden[n], ref[2, :, cols], preferred_element_type=F32)
        out_ref[:, cols] = down


def far_kernel(side, xn_ref, near_ref, far_low_ref, far_high_ref, out_ref):
    peers, count, part = out_ref.shape
    tp = peers // side
    far_pre, far_columns = far_parts(far_low_ref, far_high_ref, part)
    hidden = hidden_of(far_pre(xn_ref))
    for t in range(tp):
        cols = slice(t * part, (t + 1) * part)
        down = near_ref[:, cols] + jnp.dot(hidden, far_columns(t), preferred_element_type=F32)
        down = down.astype(BF16)
        for x in range(side):
            out_ref[x * tp + t] = down[x * count : (x + 1) * count]


def body(
    tokens,
    attn_gain,
    w_query,
    w_key,
    w_value,
    w_outgate,
    w_rates,
    head_rate,
    head_gain,
    w_out,
    state,
    mlp_gain,
    w_gate,
    w_up,
    w_down,
):
    count, part = tokens.shape
    tp = lax.axis_size("tp")
    side = 4
    width = part * tp
    size = w_query.shape[1]
    peers = side * tp
    groups = plane_groups(side, tp)

    own, rate_row, kept = pl.pallas_call(
        pack_kernel,
        out_shape=(
            pltpu.VMEM((3, UNITS, width), BF16),
            pltpu.VMEM((1, size), F32),
            pltpu.VMEM((count, part), BF16),
        ),
        in_specs=[SMEM] + [HBM] * 4,
        out_specs=(VMEM, VMEM, VMEM),
        scratch_shapes=[pltpu.VMEM((w_gate.shape[1], width), BF16)] * 3
        + [pltpu.SemaphoreType.DMA((4,))],
        compiler_params=pltpu.CompilerParams(vmem_limit_bytes=4 << 20),
        name="pack",
    )(head_rate, *in_hbm(w_gate.T, w_up.T, w_down.T, tokens))
    above = lax.ppermute(own, "kv", y_ring(1, side))
    below = lax.ppermute(own, "kv", y_ring(-1, side))
    copies = pl.pallas_call(
        spread_kernel,
        out_shape=pltpu.VMEM((tp, count, part), BF16),
        in_specs=[VMEM],
        out_specs=VMEM,
        compiler_params=pltpu.CompilerParams(vmem_limit_bytes=1 << 20),
        cost_estimate=pl.CostEstimate(
            flops=20_000_000_000, bytes_accessed=200_000, transcendentals=0
        ),
        name="spread",
    )(kept)
    tiles = lax.all_to_all(copies, "tp", 0, 0, tiled=True)
    states = pltpu.VMEM((count, size, size), F32)
    tiles, new_state = pl.pallas_call(
        attention_kernel,
        out_shape=(
            pltpu.VMEM((tp, count, part), BF16),
            pltpu.HBM((count, size, size), F32),
        ),
        in_specs=[VMEM] * 11,
        out_specs=(VMEM, HBM),
        scratch_shapes=[
            pltpu.VMEM((count, width), BF16),
            pltpu.VMEM((count, size), F32),
            pltpu.VMEM((count, size), F32),
            states,
            pltpu.SemaphoreType.DMA((4,)),
        ],
        compiler_params=pltpu.CompilerParams(vmem_limit_bytes=16 << 20),
        name="attention",
    )(
        tiles,
        attn_gain.reshape(1, width),
        w_rates.reshape(2, width),
        rate_row,
        head_gain.reshape(1, size),
        *in_vmem(
            w_query, w_key, w_value, w_outgate, w_out, state.reshape(count, size, size)
        ),
    )
    tiles = lax.all_to_all(tiles, "tp", 0, 0, tiled=True)
    half_count = count // 2
    residual, blocks = pl.pallas_call(
        residual_kernel,
        out_shape=(
            pltpu.VMEM((count, part), BF16),
            pltpu.VMEM((peers, half_count, part), BF16),
        ),
        in_specs=[VMEM, VMEM],
        out_specs=(VMEM, VMEM),
        compiler_params=pltpu.CompilerParams(vmem_limit_bytes=4 << 20),
        name="residual",
    )(tiles, kept)

    blocks, own, above, below = lax.optimization_barrier((blocks, own, above, below))
    far_low = lax.ppermute(above[:, :, : width // 2], "kv", y_ring(1, side))
    far_high = lax.ppermute(below[:, :, width // 2 :], "kv", y_ring(-1, side))
    partner = [(t, t ^ 1) for t in range(tp)]
    own_2 = lax.ppermute(own, "tp", partner)
    above_2 = lax.ppermute(above, "tp", partner)
    below_2 = lax.ppermute(below, "tp", partner)
    tiles = lax.all_to_all(
        blocks, ("kv", "tp"), 0, 0, tiled=True, axis_index_groups=groups
    )
    rows = side * half_count
    xn = pl.pallas_call(
        functools.partial(norm_kernel, side),
        out_shape=pltpu.VMEM((rows, width), BF16),
        in_specs=[VMEM] * 2,
        out_specs=VMEM,
        compiler_params=pltpu.CompilerParams(vmem_limit_bytes=4 << 20),
        name="norm",
    )(tiles, mlp_gain.reshape(1, width))
    xn, far_low, far_high = lax.optimization_barrier((xn, far_low, far_high))
    far_low_2 = lax.ppermute(far_low, "tp", partner)
    far_high_2 = lax.ppermute(far_high, "tp", partner)
    near = pl.pallas_call(
        functools.partial(near_kernel, part),
        out_shape=pltpu.VMEM((rows, width), F32),
        in_specs=[VMEM] * 9,
        out_specs=VMEM,
        compiler_params=pltpu.CompilerParams(vmem_limit_bytes=8 << 20),
        cost_estimate=pl.CostEstimate(
            flops=8_000_000_000, bytes_accessed=8_000_000, transcendentals=0
        ),
        name="near",
    )(xn, *in_vmem(own, above, below, own_2, above_2, below_2, far_low, far_high))
    tiles = pl.pallas_call(
        functools.partial(far_kernel, side),
        out_shape=pltpu.VMEM((peers, half_count, part), BF16),
        in_specs=[VMEM] * 4,
        out_specs=VMEM,
        compiler_params=pltpu.CompilerParams(vmem_limit_bytes=8 << 20),
        name="far",
    )(xn, near, *in_vmem(far_low_2, far_high_2))
    tiles = lax.all_to_all(
        tiles, ("kv", "tp"), 0, 0, tiled=True, axis_index_groups=groups
    )
    tiles = tiles.astype(F32).reshape(peers // 2, count, part)
    result = (residual.astype(F32) + jnp.sum(tiles, axis=0)).astype(BF16)
    return (result, new_state[:, None])


def solution(mesh):
    return jax.shard_map(
        body,
        mesh=mesh,
        in_specs=(
            P("kv", "tp"),
            P(),
            P(None, "tp"),
            P(None, "tp"),
            P(None, "tp"),
            P(None, "tp"),
            P(None, None, "tp"),
            P("tp"),
            P("tp"),
            P("tp", None),
            P("kv", "tp", None, None),
            P(),
            P(None, ("kv", "tp")),
            P(None, ("kv", "tp")),
            P(None, ("kv", "tp")),
        ),
        out_specs=(P("kv", "tp"), P("kv", "tp", None, None)),
        check_vma=False,
    )
```

```python
import functools

import jax
import jax.numpy as jnp
from jax import lax
from jax.experimental import pallas as pl
from jax.experimental.pallas import tpu as pltpu
from jax.sharding import PartitionSpec as P


EPS = 1e-06
F32, BF16 = jnp.float32, jnp.bfloat16
NT = (((1,), (1,)), ((), ()))
VMEM = pl.BlockSpec(memory_space=pltpu.VMEM)
SMEM = pl.BlockSpec(memory_space=pltpu.SMEM)
HBM = pl.BlockSpec(memory_space=pltpu.HBM)


def in_hbm(*arrays):
    return [pltpu.with_memory_space_constraint(a, pltpu.HBM) for a in arrays]


def in_vmem(*arrays):
    return [pltpu.with_memory_space_constraint(a, pltpu.VMEM) for a in arrays]


def y_ring(shift, side):
    return [
        (side * y + x, side * ((y + shift) % side) + x) for y in range(side) for x in range(side)
    ]


def plane_groups(side, tp):
    return [[(side * y + x) * tp + t for x in range(side) for t in range(tp)] for y in range(side)]


def silu(t):
    return t / (1.0 + jnp.exp(-t))


def norm_rows(tiles_ref, first, n_tiles, gain_ref, out_ref, at):
    rows, part = tiles_ref.shape[1:]
    total = jnp.zeros((rows, part), F32)
    for t in range(n_tiles):
        tile = tiles_ref[first + t].astype(F32)
        total = total + tile * tile
    mean = jnp.sum(total, axis=-1, keepdims=True) * (1.0 / (n_tiles * part))
    scale = lax.rsqrt(mean + EPS)
    for t in range(n_tiles):
        cols = slice(t * part, (t + 1) * part)
        tile = tiles_ref[first + t].astype(F32)
        out_ref[at : at + rows, cols] = (tile * scale * gain_ref[0:1, cols]).astype(BF16)


def attention_kernel(
    tiles_ref, gain_ref, wr_ref, rate_ref, head_gain_ref, wq_ref, wk_ref, wv_ref, wg_ref, wo_ref,
    state_ref, out_ref, new_state_hbm, xn_ref, u_ref, w_ref, new_state_ref, out_sems,
):
    tp, count, part = tiles_ref.shape
    size = wq_ref.shape[1]
    norm_rows(tiles_ref, 0, tp, gain_ref, xn_ref, 0)
    xn = xn_ref[...]
    rates = lax.dot_general(xn, wr_ref[...], NT, preferred_element_type=F32)
    query = jnp.dot(xn, wq_ref[...], preferred_element_type=F32)
    key = jnp.dot(xn, wk_ref[...], preferred_element_type=F32)
    strength = 1.0 / (1.0 + jnp.exp(-rates[:, 0:1]))
    decay = rates[:, 1:2]
    softplus = jnp.maximum(decay, 0.0) + jnp.log(1.0 + jnp.exp(-jnp.abs(decay)))
    fade = jnp.exp(-rate_ref[...] * softplus)
    q = query * lax.rsqrt(jnp.sum(query * query, -1, keepdims=True) + EPS) * size**-0.5
    k = key * lax.rsqrt(jnp.sum(key * key, -1, keepdims=True) + EPS)
    q_high, k_high = q.astype(BF16), k.astype(BF16)
    q_low = (q - q_high.astype(F32)).astype(BF16)
    k_low = (k - k_high.astype(F32)).astype(BF16)
    probes = jnp.concatenate([k_high, k_low, q_high, q_low], axis=0)
    for b in range(count):
        read = jnp.dot(probes, state_ref[b].astype(BF16), preferred_element_type=F32)
        u_ref[b : b + 1, :] = read[b : b + 1] + read[count + b : count + b + 1]
        w_ref[b : b + 1, :] = read[2 * count + b : 2 * count + b + 1] + read[
            3 * count + b : 3 * count + b + 1
        ]
    value = jnp.dot(xn, wv_ref[...], preferred_element_type=F32)
    gate_in = jnp.dot(xn, wg_ref[...], preferred_element_type=F32)
    fresh = strength * (value - fade * u_ref[...])
    readout = fade * w_ref[...] + jnp.sum(q * k, -1, keepdims=True) * fresh
    k_columns = k.T
    stores = []
    for b in range(count):
        new_state_ref[b] = (
            fade[b : b + 1, :] * state_ref[b] + k_columns[:, b : b + 1] * fresh[b : b + 1, :]
        )
        if b % 4 == 3:
            rows = pl.ds(b - 3, 4)
            stores.append(
                pltpu.make_async_copy(
                    new_state_ref.at[rows], new_state_hbm.at[rows], out_sems.at[b // 4]
                )
            )
            stores[-1].start()
    scale = lax.rsqrt(jnp.mean(readout * readout, -1, keepdims=True) + EPS)
    mixed = (readout * scale * head_gain_ref[...] * silu(gate_in)).astype(BF16)
    for t in range(tp):
        cols = slice(t * part, (t + 1) * part)
        out_ref[t] = jnp.dot(mixed, wo_ref[:, cols], preferred_element_type=F32).astype(BF16)
    for store in stores:
        store.wait()


def residual_kernel(tiles_ref, tokens_ref, out_ref, blocks_ref):
    total = tokens_ref[...].astype(F32)
    for t in range(tiles_ref.shape[0]):
        total = total + tiles_ref[t].astype(F32)
    residual = total.astype(BF16)
    out_ref[...] = residual
    rows = blocks_ref.shape[1]
    for b in range(blocks_ref.shape[0]):
        at = (b % 2) * rows
        blocks_ref[b] = residual[at : at + rows]


def pack_kernel(
    rate_ref, gate_hbm, up_hbm, down_hbm, tokens_hbm, own_ref, rate_row_ref, tokens_ref, sems
):
    loads = [pltpu.make_async_copy(tokens_hbm, tokens_ref, sems.at[3])]
    for n, source in enumerate((gate_hbm, up_hbm, down_hbm)):
        loads.append(pltpu.make_async_copy(source, own_ref.at[n], sems.at[n]))
    for load in loads:
        load.start()
    rate_row_ref[...] = jnp.full(rate_row_ref.shape, rate_ref[0], F32)
    for load in loads:
        load.wait()


def spread_kernel(tokens_ref, copies_ref):
    for b in range(copies_ref.shape[0]):
        copies_ref[b] = tokens_ref[...]


def hidden_of(xn, ref):
    gate_pre = lax.dot_general(xn, ref[0], NT, preferred_element_type=F32)
    up_pre = lax.dot_general(xn, ref[1], NT, preferred_element_type=F32)
    return (silu(gate_pre) * up_pre).astype(BF16)


def hidden_of_halves(xn_ref, low_ref, high_ref):
    half = low_ref.shape[2]
    low, high = xn_ref[:, :half], xn_ref[:, half:]
    pre = [
        lax.dot_general(low, low_ref[n], NT, preferred_element_type=F32)
        + lax.dot_general(high, high_ref[n], NT, preferred_element_type=F32)
        for n in range(2)
    ]
    return (silu(pre[0]) * pre[1]).astype(BF16)


def norm_kernel(side, tiles_ref, gain_ref, xn_ref):
    peers, count, _ = tiles_ref.shape
    tp = peers // side
    for x in range(side):
        norm_rows(tiles_ref, x * tp, tp, gain_ref, xn_ref, x * count)


def near_kernel(xn_ref, *refs):
    *whole, far_low_ref, far_high_ref, out_ref = refs
    half = far_low_ref.shape[2]
    xn = xn_ref[...]
    hidden = [hidden_of(xn, ref) for ref in whole]
    far = hidden_of_halves(xn_ref, far_low_ref, far_high_ref)
    out_ref[:, :half] = jnp.dot(far, far_low_ref[2], preferred_element_type=F32)
    out_ref[:, half:] = jnp.dot(far, far_high_ref[2], preferred_element_type=F32)
    for n, ref in enumerate(whole):
        out_ref[...] += jnp.dot(hidden[n], ref[2], preferred_element_type=F32)


def far_kernel(side, xn_ref, near_ref, far_low_ref, far_high_ref, out_ref):
    peers, count, part = out_ref.shape
    tp = peers // side
    half = far_low_ref.shape[2]
    hidden = hidden_of_halves(xn_ref, far_low_ref, far_high_ref)
    for t in range(tp):
        cols = slice(t * part, (t + 1) * part)
        if (t + 1) * part <= half:
            weight = far_low_ref[2, :, cols]
        else:
            weight = far_high_ref[2, :, t * part - half : (t + 1) * part - half]
        down = near_ref[:, cols] + jnp.dot(hidden, weight, preferred_element_type=F32)
        down = down.astype(BF16)
        for x in range(side):
            out_ref[x * tp + t] = down[x * count : (x + 1) * count]


def body(
    tokens,
    attn_gain,
    w_query,
    w_key,
    w_value,
    w_outgate,
    w_rates,
    head_rate,
    head_gain,
    w_out,
    state,
    mlp_gain,
    w_gate,
    w_up,
    w_down,
):
    count, part = tokens.shape
    tp = lax.axis_size("tp")
    side = 4
    width = part * tp
    size = w_query.shape[1]
    peers = side * tp
    groups = plane_groups(side, tp)

    own, rate_row, kept = pl.pallas_call(
        pack_kernel,
        out_shape=(
            pltpu.VMEM((3, w_gate.shape[1], width), BF16),
            pltpu.VMEM((1, size), F32),
            pltpu.VMEM((count, part), BF16),
        ),
        in_specs=[SMEM] + [HBM] * 4,
        out_specs=(VMEM, VMEM, VMEM),
        scratch_shapes=[pltpu.SemaphoreType.DMA((4,))],
        compiler_params=pltpu.CompilerParams(vmem_limit_bytes=4 << 20),
        name="pack",
    )(head_rate, *in_hbm(w_gate.T, w_up.T, w_down.T, tokens))
    above = lax.ppermute(own, "kv", y_ring(1, side))
    below = lax.ppermute(own, "kv", y_ring(-1, side))
    copies = pl.pallas_call(
        spread_kernel,
        out_shape=pltpu.VMEM((tp, count, part), BF16),
        in_specs=[VMEM],
        out_specs=VMEM,
        compiler_params=pltpu.CompilerParams(vmem_limit_bytes=1 << 20),
        cost_estimate=pl.CostEstimate(
            flops=20_000_000_000, bytes_accessed=200_000, transcendentals=0
        ),
        name="spread",
    )(kept)
    tiles = lax.all_to_all(copies, "tp", 0, 0, tiled=True)
    states = pltpu.VMEM((count, size, size), F32)
    tiles, new_state = pl.pallas_call(
        attention_kernel,
        out_shape=(
            pltpu.VMEM((tp, count, part), BF16),
            pltpu.HBM((count, size, size), F32),
        ),
        in_specs=[VMEM] * 11,
        out_specs=(VMEM, HBM),
        scratch_shapes=[
            pltpu.VMEM((count, width), BF16),
            pltpu.VMEM((count, size), F32),
            pltpu.VMEM((count, size), F32),
            states,
            pltpu.SemaphoreType.DMA((4,)),
        ],
        compiler_params=pltpu.CompilerParams(vmem_limit_bytes=16 << 20),
        name="attention",
    )(
        tiles,
        attn_gain.reshape(1, width),
        w_rates.reshape(2, width),
        rate_row,
        head_gain.reshape(1, size),
        *in_vmem(
            w_query, w_key, w_value, w_outgate, w_out, state.reshape(count, size, size)
        ),
    )
    tiles = lax.all_to_all(tiles, "tp", 0, 0, tiled=True)
    half_count = count // 2
    residual, blocks = pl.pallas_call(
        residual_kernel,
        out_shape=(
            pltpu.VMEM((count, part), BF16),
            pltpu.VMEM((peers, half_count, part), BF16),
        ),
        in_specs=[VMEM, VMEM],
        out_specs=(VMEM, VMEM),
        compiler_params=pltpu.CompilerParams(vmem_limit_bytes=4 << 20),
        name="residual",
    )(tiles, kept)

    blocks, own, above, below = lax.optimization_barrier((blocks, own, above, below))
    far_low = lax.ppermute(above[:, :, : width // 2], "kv", y_ring(1, side))
    far_high = lax.ppermute(below[:, :, width // 2 :], "kv", y_ring(-1, side))
    partner = [(t, t ^ 1) for t in range(tp)]
    own_2 = lax.ppermute(own, "tp", partner)
    above_2 = lax.ppermute(above, "tp", partner)
    below_2 = lax.ppermute(below, "tp", partner)
    tiles = lax.all_to_all(
        blocks, ("kv", "tp"), 0, 0, tiled=True, axis_index_groups=groups
    )
    rows = side * half_count
    xn = pl.pallas_call(
        functools.partial(norm_kernel, side),
        out_shape=pltpu.VMEM((rows, width), BF16),
        in_specs=[VMEM] * 2,
        out_specs=VMEM,
        compiler_params=pltpu.CompilerParams(vmem_limit_bytes=4 << 20),
        name="norm",
    )(tiles, mlp_gain.reshape(1, width))
    xn, far_low, far_high = lax.optimization_barrier((xn, far_low, far_high))
    far_low_2 = lax.ppermute(far_low, "tp", partner)
    far_high_2 = lax.ppermute(far_high, "tp", partner)
    near = pl.pallas_call(
        near_kernel,
        out_shape=pltpu.VMEM((rows, width), F32),
        in_specs=[VMEM] * 9,
        out_specs=VMEM,
        compiler_params=pltpu.CompilerParams(vmem_limit_bytes=8 << 20),
        cost_estimate=pl.CostEstimate(
            flops=8_000_000_000, bytes_accessed=8_000_000, transcendentals=0
        ),
        name="near",
    )(xn, *in_vmem(own, above, below, own_2, above_2, below_2, far_low, far_high))
    tiles = pl.pallas_call(
        functools.partial(far_kernel, side),
        out_shape=pltpu.VMEM((peers, half_count, part), BF16),
        in_specs=[VMEM] * 4,
        out_specs=VMEM,
        compiler_params=pltpu.CompilerParams(vmem_limit_bytes=8 << 20),
        name="far",
    )(xn, near, *in_vmem(far_low_2, far_high_2))
    tiles = lax.all_to_all(
        tiles, ("kv", "tp"), 0, 0, tiled=True, axis_index_groups=groups
    )
    tiles = tiles.astype(F32).reshape(peers // 2, count, part)
    result = (residual.astype(F32) + jnp.sum(tiles, axis=0)).astype(BF16)
    return (result, new_state[:, None])


def solution(mesh):
    return jax.shard_map(
        body,
        mesh=mesh,
        in_specs=(
            P("kv", "tp"),
            P(),
            P(None, "tp"),
            P(None, "tp"),
            P(None, "tp"),
            P(None, "tp"),
            P(None, None, "tp"),
            P("tp"),
            P("tp"),
            P("tp", None),
            P("kv", "tp", None, None),
            P(),
            P(None, ("kv", "tp")),
            P(None, ("kv", "tp")),
            P(None, ("kv", "tp")),
        ),
        out_specs=(P("kv", "tp"), P("kv", "tp", None, None)),
        check_vma=False,
    )
```

```python
import functools

import jax
import jax.numpy as jnp
from jax import lax
from jax.experimental import pallas as pl
from jax.experimental.pallas import tpu as pltpu
from jax.sharding import PartitionSpec as P


EPS = 1e-06
F32, BF16 = jnp.float32, jnp.bfloat16
NT = (((1,), (1,)), ((), ()))
VMEM = pl.BlockSpec(memory_space=pltpu.VMEM)
SMEM = pl.BlockSpec(memory_space=pltpu.SMEM)
HBM = pl.BlockSpec(memory_space=pltpu.HBM)


def in_hbm(*arrays):
    return [pltpu.with_memory_space_constraint(a, pltpu.HBM) for a in arrays]


def in_vmem(*arrays):
    return [pltpu.with_memory_space_constraint(a, pltpu.VMEM) for a in arrays]


def y_ring(shift, side, tp):
    return [
        ((side * y + x) * tp + t, (side * ((y + (1 - 2 * (t % 2)) * shift) % side) + x) * tp + t)
        for y in range(side)
        for x in range(side)
        for t in range(tp)
    ]


def ring_order(tp):
    return list(range(tp))


def plane_order(side, tp):
    return [(x, t) for x in range(side) for t in range(tp)]


def plane_groups(side, tp):
    return [[(side * y + x) * tp + t for x, t in plane_order(side, tp)] for y in range(side)]


def silu(t):
    return t / (1.0 + jnp.exp(-t))


def norm_rows(tiles_ref, places, gain_ref, out_ref, at):
    rows, part = tiles_ref.shape[1:]
    total = jnp.zeros((rows, part), F32)
    for place in places:
        tile = tiles_ref[place].astype(F32)
        total = total + tile * tile
    mean = jnp.sum(total, axis=-1, keepdims=True) * (1.0 / (len(places) * part))
    scale = lax.rsqrt(mean + EPS)
    for t, place in enumerate(places):
        cols = slice(t * part, (t + 1) * part)
        tile = tiles_ref[place].astype(F32)
        out_ref[at : at + rows, cols] = (tile * scale * gain_ref[0:1, cols]).astype(BF16)


def attention_kernel(
    tiles_ref, gain_ref, wr_ref, rate_ref, head_gain_ref, wq_ref, wk_ref, wv_ref, wg_ref, wo_ref,
    state_ref, out_ref, new_state_hbm, xn_ref, u_ref, w_ref, new_state_ref, out_sems,
):
    tp, count, part = tiles_ref.shape
    size = wq_ref.shape[1]
    order = ring_order(tp)
    norm_rows(tiles_ref, [order.index(t) for t in range(tp)], gain_ref, xn_ref, 0)
    xn = xn_ref[...]
    rates = lax.dot_general(xn, wr_ref[...], NT, preferred_element_type=F32)
    query = jnp.dot(xn, wq_ref[...], preferred_element_type=F32)
    key = jnp.dot(xn, wk_ref[...], preferred_element_type=F32)
    strength = 1.0 / (1.0 + jnp.exp(-rates[:, 0:1]))
    decay = rates[:, 1:2]
    softplus = jnp.maximum(decay, 0.0) + jnp.log(1.0 + jnp.exp(-jnp.abs(decay)))
    fade = jnp.exp(-rate_ref[...] * softplus)
    q = query * lax.rsqrt(jnp.sum(query * query, -1, keepdims=True) + EPS) * size**-0.5
    k = key * lax.rsqrt(jnp.sum(key * key, -1, keepdims=True) + EPS)
    q_high, k_high = q.astype(BF16), k.astype(BF16)
    q_low = (q - q_high.astype(F32)).astype(BF16)
    k_low = (k - k_high.astype(F32)).astype(BF16)
    probes = jnp.concatenate([k_high, k_low, q_high, q_low], axis=0)
    for b in range(count):
        read = jnp.dot(probes, state_ref[b].astype(BF16), preferred_element_type=F32)
        u_ref[b : b + 1, :] = read[b : b + 1] + read[count + b : count + b + 1]
        w_ref[b : b + 1, :] = read[2 * count + b : 2 * count + b + 1] + read[
            3 * count + b : 3 * count + b + 1
        ]
    value = jnp.dot(xn, wv_ref[...], preferred_element_type=F32)
    gate_in = jnp.dot(xn, wg_ref[...], preferred_element_type=F32)
    fresh = strength * (value - fade * u_ref[...])
    readout = fade * w_ref[...] + jnp.sum(q * k, -1, keepdims=True) * fresh
    k_columns = k.T
    stores = []
    for b in range(count):
        new_state_ref[b] = (
            fade[b : b + 1, :] * state_ref[b] + k_columns[:, b : b + 1] * fresh[b : b + 1, :]
        )
        if b % 4 == 3:
            rows = pl.ds(b - 3, 4)
            stores.append(
                pltpu.make_async_copy(
                    new_state_ref.at[rows], new_state_hbm.at[rows], out_sems.at[b // 4]
                )
            )
            stores[-1].start()
    scale = lax.rsqrt(jnp.mean(readout * readout, -1, keepdims=True) + EPS)
    mixed = (readout * scale * head_gain_ref[...] * silu(gate_in)).astype(BF16)
    for n, t in enumerate(order):
        cols = slice(t * part, (t + 1) * part)
        out_ref[n] = jnp.dot(mixed, wo_ref[:, cols], preferred_element_type=F32).astype(BF16)
    for store in stores:
        store.wait()


def residual_kernel(order, tiles_ref, tokens_ref, out_ref, blocks_ref):
    total = tokens_ref[...].astype(F32)
    for t in range(tiles_ref.shape[0]):
        total = total + tiles_ref[t].astype(F32)
    residual = total.astype(BF16)
    out_ref[...] = residual
    rows = blocks_ref.shape[1]
    for n, (_, t) in enumerate(order):
        at = (t % 2) * rows
        blocks_ref[n] = residual[at : at + rows]


def pack_kernel(
    rate_ref, gate_hbm, up_hbm, down_hbm, tokens_hbm, own_ref, rate_row_ref, tokens_ref, sems
):
    loads = [pltpu.make_async_copy(tokens_hbm, tokens_ref, sems.at[3])]
    for n, source in enumerate((gate_hbm, up_hbm, down_hbm)):
        loads.append(pltpu.make_async_copy(source, own_ref.at[n], sems.at[n]))
    for load in loads:
        load.start()
    rate_row_ref[...] = jnp.full(rate_row_ref.shape, rate_ref[0], F32)
    for load in loads:
        load.wait()


def spread_kernel(tokens_ref, copies_ref):
    for b in range(copies_ref.shape[0]):
        copies_ref[b] = tokens_ref[...]


def hidden_of(xn, ref):
    gate_pre = lax.dot_general(xn, ref[0], NT, preferred_element_type=F32)
    up_pre = lax.dot_general(xn, ref[1], NT, preferred_element_type=F32)
    return (silu(gate_pre) * up_pre).astype(BF16)


def norm_kernel(side, order, tiles_ref, gain_ref, xn_ref):
    peers, count, _ = tiles_ref.shape
    tp = peers // side
    for x in range(side):
        places = [order.index((x, t)) for t in range(tp)]
        norm_rows(tiles_ref, places, gain_ref, xn_ref, x * count)


def last_kernel(order, tiles_ref, residual_ref, out_ref):
    rows = tiles_ref.shape[1]
    for half in range(2):
        at = slice(half * rows, (half + 1) * rows)
        total = residual_ref[at].astype(F32)
        for n, (_, t) in enumerate(order):
            if t % 2 == half:
                total = total + tiles_ref[n].astype(F32)
        out_ref[at] = total.astype(BF16)


def near_kernel(xn_ref, *refs):
    *blocks, out_ref = refs
    xn = xn_ref[...]
    hidden = [hidden_of(xn, ref) for ref in blocks]
    for n, ref in enumerate(blocks):
        down = jnp.dot(hidden[n], ref[2], preferred_element_type=F32)
        out_ref[...] = down if n == 0 else out_ref[...] + down


def far_kernel(side, order, xn_ref, near_ref, far_ref, out_ref):
    peers, count, part = out_ref.shape
    tp = peers // side
    hidden = hidden_of(xn_ref[...], far_ref)
    for t in range(tp):
        cols = slice(t * part, (t + 1) * part)
        down = jnp.dot(hidden, far_ref[2, :, cols], preferred_element_type=F32)
        down = (near_ref[:, cols] + down).astype(BF16)
        for x in range(side):
            out_ref[order.index((x, t))] = down[x * count : (x + 1) * count]


def body(
    tokens,
    attn_gain,
    w_query,
    w_key,
    w_value,
    w_outgate,
    w_rates,
    head_rate,
    head_gain,
    w_out,
    state,
    mlp_gain,
    w_gate,
    w_up,
    w_down,
):
    count, part = tokens.shape
    tp = lax.axis_size("tp")
    side = 4
    width = part * tp
    size = w_query.shape[1]
    peers = side * tp
    groups = plane_groups(side, tp)
    order = plane_order(side, tp)
    ring = [ring_order(tp)]

    own, rate_row, kept = pl.pallas_call(
        pack_kernel,
        out_shape=(
            pltpu.VMEM((3, w_gate.shape[1], width), BF16),
            pltpu.VMEM((1, size), F32),
            pltpu.VMEM((count, part), BF16),
        ),
        in_specs=[SMEM] + [HBM] * 4,
        out_specs=(VMEM, VMEM, VMEM),
        scratch_shapes=[pltpu.SemaphoreType.DMA((4,))],
        compiler_params=pltpu.CompilerParams(vmem_limit_bytes=4 << 20),
        name="pack",
    )(head_rate, *in_hbm(w_gate.T, w_up.T, w_down.T, tokens))
    above = lax.ppermute(own, ("kv", "tp"), y_ring(1, side, tp))
    below = lax.ppermute(own, ("kv", "tp"), y_ring(-1, side, tp))
    copies = pl.pallas_call(
        spread_kernel,
        out_shape=pltpu.VMEM((tp, count, part), BF16),
        in_specs=[VMEM],
        out_specs=VMEM,
        compiler_params=pltpu.CompilerParams(vmem_limit_bytes=1 << 20),
        cost_estimate=pl.CostEstimate(
            flops=20_000_000_000, bytes_accessed=200_000, transcendentals=0
        ),
        name="spread",
    )(kept)
    tiles = lax.all_to_all(copies, "tp", 0, 0, tiled=True, axis_index_groups=ring)
    states = pltpu.VMEM((count, size, size), F32)
    tiles, new_state = pl.pallas_call(
        attention_kernel,
        out_shape=(
            pltpu.VMEM((tp, count, part), BF16),
            pltpu.HBM((count, size, size), F32),
        ),
        in_specs=[VMEM] * 11,
        out_specs=(VMEM, HBM),
        scratch_shapes=[
            pltpu.VMEM((count, width), BF16),
            pltpu.VMEM((count, size), F32),
            pltpu.VMEM((count, size), F32),
            states,
            pltpu.SemaphoreType.DMA((4,)),
        ],
        compiler_params=pltpu.CompilerParams(vmem_limit_bytes=16 << 20),
        name="attention",
    )(
        tiles,
        attn_gain.reshape(1, width),
        w_rates.reshape(2, width),
        rate_row,
        head_gain.reshape(1, size),
        *in_vmem(
            w_query, w_key, w_value, w_outgate, w_out, state.reshape(count, size, size)
        ),
    )
    tiles = lax.all_to_all(tiles, "tp", 0, 0, tiled=True, axis_index_groups=ring)
    half_count = count // 2
    residual, blocks = pl.pallas_call(
        functools.partial(residual_kernel, order),
        out_shape=(
            pltpu.VMEM((count, part), BF16),
            pltpu.VMEM((peers, half_count, part), BF16),
        ),
        in_specs=[VMEM, VMEM],
        out_specs=(VMEM, VMEM),
        compiler_params=pltpu.CompilerParams(vmem_limit_bytes=4 << 20),
        name="residual",
    )(tiles, kept)

    blocks, own, above, below = lax.optimization_barrier((blocks, own, above, below))
    far = lax.ppermute(above, ("kv", "tp"), y_ring(1, side, tp))
    partner = [(t, t ^ 1) for t in range(tp)]
    own_2 = lax.ppermute(own, "tp", partner)
    above_2 = lax.ppermute(above, "tp", partner)
    below_2 = lax.ppermute(below, "tp", partner)
    tiles = lax.all_to_all(
        blocks, ("kv", "tp"), 0, 0, tiled=True, axis_index_groups=groups
    )
    rows = side * half_count
    xn = pl.pallas_call(
        functools.partial(norm_kernel, side, order),
        out_shape=pltpu.VMEM((rows, width), BF16),
        in_specs=[VMEM] * 2,
        out_specs=VMEM,
        compiler_params=pltpu.CompilerParams(vmem_limit_bytes=4 << 20),
        name="norm",
    )(tiles, mlp_gain.reshape(1, width))
    xn, far = lax.optimization_barrier((xn, far))
    far_2 = lax.ppermute(far, "tp", partner)
    near = pl.pallas_call(
        near_kernel,
        out_shape=pltpu.VMEM((rows, width), F32),
        in_specs=[VMEM] * 8,
        out_specs=VMEM,
        compiler_params=pltpu.CompilerParams(vmem_limit_bytes=8 << 20),
        cost_estimate=pl.CostEstimate(
            flops=8_000_000_000, bytes_accessed=8_000_000, transcendentals=0
        ),
        name="near",
    )(xn, *in_vmem(own, above, below, own_2, above_2, below_2, far))
    tiles = pl.pallas_call(
        functools.partial(far_kernel, side, order),
        out_shape=pltpu.VMEM((peers, half_count, part), BF16),
        in_specs=[VMEM] * 3,
        out_specs=VMEM,
        compiler_params=pltpu.CompilerParams(vmem_limit_bytes=8 << 20),
        name="far",
    )(xn, near, *in_vmem(far_2))
    tiles = lax.all_to_all(
        tiles, ("kv", "tp"), 0, 0, tiled=True, axis_index_groups=groups
    )
    result = pl.pallas_call(
        functools.partial(last_kernel, order),
        out_shape=jax.ShapeDtypeStruct((count, part), BF16),
        in_specs=[VMEM] * 2,
        out_specs=VMEM,
        compiler_params=pltpu.CompilerParams(vmem_limit_bytes=1 << 20),
        name="last",
    )(tiles, residual)
    return (result, new_state[:, None])


def solution(mesh):
    return jax.shard_map(
        body,
        mesh=mesh,
        in_specs=(
            P("kv", "tp"),
            P(),
            P(None, "tp"),
            P(None, "tp"),
            P(None, "tp"),
            P(None, "tp"),
            P(None, None, "tp"),
            P("tp"),
            P("tp"),
            P("tp", None),
            P("kv", "tp", None, None),
            P(),
            P(None, ("kv", "tp")),
            P(None, ("kv", "tp")),
            P(None, ("kv", "tp")),
        ),
        out_specs=(P("kv", "tp"), P("kv", "tp", None, None)),
        check_vma=False,
    )
```

```python
import functools

import jax
import jax.numpy as jnp
from jax import lax
from jax.experimental import pallas as pl
from jax.experimental.pallas import tpu as pltpu
from jax.sharding import PartitionSpec as P


EPS = 1e-06
F32, BF16 = jnp.float32, jnp.bfloat16
NT = (((1,), (1,)), ((), ()))
VMEM = pl.BlockSpec(memory_space=pltpu.VMEM)
SMEM = pl.BlockSpec(memory_space=pltpu.SMEM)
HBM = pl.BlockSpec(memory_space=pltpu.HBM)


def in_hbm(*arrays):
    return [pltpu.with_memory_space_constraint(a, pltpu.HBM) for a in arrays]


def in_vmem(*arrays):
    return [pltpu.with_memory_space_constraint(a, pltpu.VMEM) for a in arrays]


def y_ring(shift, side, tp):
    return [
        ((side * y + x) * tp + t, (side * ((y + (1 - 2 * (t % 2)) * shift) % side) + x) * tp + t)
        for y in range(side)
        for x in range(side)
        for t in range(tp)
    ]


def ring_order(tp):
    return list(range(tp))


def plane_order(side, tp):
    return [(x, t) for x in range(side) for t in range(tp)]


def plane_groups(side, tp):
    return [[(side * y + x) * tp + t for x, t in plane_order(side, tp)] for y in range(side)]


def silu(t):
    return t / (1.0 + jnp.exp(-t))


def norm_rows(tiles_ref, places, gain_ref, out_ref, at):
    rows, part = tiles_ref.shape[1:]
    total = jnp.zeros((rows, part), F32)
    for place in places:
        tile = tiles_ref[place].astype(F32)
        total = total + tile * tile
    mean = jnp.sum(total, axis=-1, keepdims=True) * (1.0 / (len(places) * part))
    scale = lax.rsqrt(mean + EPS)
    for t, place in enumerate(places):
        cols = slice(t * part, (t + 1) * part)
        tile = tiles_ref[place].astype(F32)
        out_ref[at : at + rows, cols] = (tile * scale * gain_ref[0:1, cols]).astype(BF16)


def attention_kernel(
    tiles_ref, gain_ref, wr_ref, rate_ref, head_gain_ref, wq_ref, wk_ref, wv_ref, wg_ref, wo_ref,
    state_ref, out_ref, new_state_hbm, xn_ref, u_ref, w_ref, new_state_ref, out_sems,
):
    tp, count, part = tiles_ref.shape
    size = wq_ref.shape[1]
    order = ring_order(tp)
    norm_rows(tiles_ref, [order.index(t) for t in range(tp)], gain_ref, xn_ref, 0)
    xn = xn_ref[...]
    rates = lax.dot_general(xn, wr_ref[...], NT, preferred_element_type=F32)
    query = jnp.dot(xn, wq_ref[...], preferred_element_type=F32)
    key = jnp.dot(xn, wk_ref[...], preferred_element_type=F32)
    strength = 1.0 / (1.0 + jnp.exp(-rates[:, 0:1]))
    decay = rates[:, 1:2]
    softplus = jnp.maximum(decay, 0.0) + jnp.log(1.0 + jnp.exp(-jnp.abs(decay)))
    fade = jnp.exp(-rate_ref[...] * softplus)
    q = query * lax.rsqrt(jnp.sum(query * query, -1, keepdims=True) + EPS) * size**-0.5
    k = key * lax.rsqrt(jnp.sum(key * key, -1, keepdims=True) + EPS)
    q_high, k_high = q.astype(BF16), k.astype(BF16)
    q_low = (q - q_high.astype(F32)).astype(BF16)
    k_low = (k - k_high.astype(F32)).astype(BF16)
    probes = jnp.concatenate([k_high, k_low, q_high, q_low], axis=0)
    for b in range(count):
        read = jnp.dot(probes, state_ref[b].astype(BF16), preferred_element_type=F32)
        u_ref[b : b + 1, :] = read[b : b + 1] + read[count + b : count + b + 1]
        w_ref[b : b + 1, :] = read[2 * count + b : 2 * count + b + 1] + read[
            3 * count + b : 3 * count + b + 1
        ]
    value = jnp.dot(xn, wv_ref[...], preferred_element_type=F32)
    gate_in = jnp.dot(xn, wg_ref[...], preferred_element_type=F32)
    fresh = strength * (value - fade * u_ref[...])
    readout = fade * w_ref[...] + jnp.sum(q * k, -1, keepdims=True) * fresh
    k_columns = k.T
    stores = []
    for b in range(count):
        new_state_ref[b] = (
            fade[b : b + 1, :] * state_ref[b] + k_columns[:, b : b + 1] * fresh[b : b + 1, :]
        )
        if b % 4 == 3:
            rows = pl.ds(b - 3, 4)
            stores.append(
                pltpu.make_async_copy(
                    new_state_ref.at[rows], new_state_hbm.at[rows], out_sems.at[b // 4]
                )
            )
            stores[-1].start()
    scale = lax.rsqrt(jnp.mean(readout * readout, -1, keepdims=True) + EPS)
    mixed = (readout * scale * head_gain_ref[...] * silu(gate_in)).astype(BF16)
    for n, t in enumerate(order):
        cols = slice(t * part, (t + 1) * part)
        out_ref[n] = jnp.dot(mixed, wo_ref[:, cols], preferred_element_type=F32).astype(BF16)
    for store in stores:
        store.wait()


def residual_kernel(order, tiles_ref, tokens_ref, out_ref, blocks_ref):
    total = tokens_ref[...].astype(F32)
    for t in range(tiles_ref.shape[0]):
        total = total + tiles_ref[t].astype(F32)
    residual = total.astype(BF16)
    out_ref[...] = residual
    rows = blocks_ref.shape[1]
    for n, (_, t) in enumerate(order):
        at = (t % 2) * rows
        blocks_ref[n] = residual[at : at + rows]


def pack_kernel(
    rate_ref, gate_hbm, up_hbm, down_hbm, tokens_hbm, own_ref, rate_row_ref, tokens_ref, sems
):
    loads = [pltpu.make_async_copy(tokens_hbm, tokens_ref, sems.at[3])]
    for n, source in enumerate((gate_hbm, up_hbm, down_hbm)):
        loads.append(pltpu.make_async_copy(source, own_ref.at[n], sems.at[n]))
    for load in loads:
        load.start()
    rate_row_ref[...] = jnp.full(rate_row_ref.shape, rate_ref[0], F32)
    for load in loads:
        load.wait()


def spread_kernel(tokens_ref, copies_ref):
    for b in range(copies_ref.shape[0]):
        copies_ref[b] = tokens_ref[...]


def hidden_of(xn, ref):
    gate_pre = lax.dot_general(xn, ref[0], NT, preferred_element_type=F32)
    up_pre = lax.dot_general(xn, ref[1], NT, preferred_element_type=F32)
    return (silu(gate_pre) * up_pre).astype(BF16)


def last_kernel(order, tiles_ref, residual_ref, out_ref):
    rows = tiles_ref.shape[1]
    for half in range(2):
        at = slice(half * rows, (half + 1) * rows)
        total = residual_ref[at].astype(F32)
        for n, (_, t) in enumerate(order):
            if t % 2 == half:
                total = total + tiles_ref[n].astype(F32)
        out_ref[at] = total.astype(BF16)


def near_kernel(side, order, tiles_ref, gain_ref, *refs):
    *blocks, xn_ref, out_ref = refs
    peers, count, _ = tiles_ref.shape
    tp = peers // side
    for x in range(side):
        places = [order.index((x, t)) for t in range(tp)]
        norm_rows(tiles_ref, places, gain_ref, xn_ref, x * count)
    xn = xn_ref[...]
    hidden = [hidden_of(xn, ref) for ref in blocks]
    for n, ref in enumerate(blocks):
        down = jnp.dot(hidden[n], ref[2], preferred_element_type=F32)
        out_ref[...] = down if n == 0 else out_ref[...] + down


def far_kernel(side, order, xn_ref, near_ref, far_ref, out_ref):
    peers, count, part = out_ref.shape
    tp = peers // side
    hidden = hidden_of(xn_ref[...], far_ref)
    for t in range(tp):
        cols = slice(t * part, (t + 1) * part)
        down = jnp.dot(hidden, far_ref[2, :, cols], preferred_element_type=F32)
        down = (near_ref[:, cols] + down).astype(BF16)
        for x in range(side):
            out_ref[order.index((x, t))] = down[x * count : (x + 1) * count]


def body(
    tokens,
    attn_gain,
    w_query,
    w_key,
    w_value,
    w_outgate,
    w_rates,
    head_rate,
    head_gain,
    w_out,
    state,
    mlp_gain,
    w_gate,
    w_up,
    w_down,
):
    count, part = tokens.shape
    tp = lax.axis_size("tp")
    side = 4
    width = part * tp
    size = w_query.shape[1]
    peers = side * tp
    groups = plane_groups(side, tp)
    order = plane_order(side, tp)
    ring = [ring_order(tp)]

    own, rate_row, kept = pl.pallas_call(
        pack_kernel,
        out_shape=(
            pltpu.VMEM((3, w_gate.shape[1], width), BF16),
            pltpu.VMEM((1, size), F32),
            pltpu.VMEM((count, part), BF16),
        ),
        in_specs=[SMEM] + [HBM] * 4,
        out_specs=(VMEM, VMEM, VMEM),
        scratch_shapes=[pltpu.SemaphoreType.DMA((4,))],
        compiler_params=pltpu.CompilerParams(vmem_limit_bytes=4 << 20),
        name="pack",
    )(head_rate, *in_hbm(w_gate.T, w_up.T, w_down.T, tokens))
    partner = [(t, t ^ 1) for t in range(tp)]
    own_2 = lax.ppermute(own, "tp", partner)
    above = lax.ppermute(own, ("kv", "tp"), y_ring(1, side, tp))
    below = lax.ppermute(own, ("kv", "tp"), y_ring(-1, side, tp))
    copies = pl.pallas_call(
        spread_kernel,
        out_shape=pltpu.VMEM((tp, count, part), BF16),
        in_specs=[VMEM],
        out_specs=VMEM,
        compiler_params=pltpu.CompilerParams(vmem_limit_bytes=1 << 20),
        cost_estimate=pl.CostEstimate(
            flops=20_000_000_000, bytes_accessed=200_000, transcendentals=0
        ),
        name="spread",
    )(kept)
    tiles = lax.all_to_all(copies, "tp", 0, 0, tiled=True, axis_index_groups=ring)
    states = pltpu.VMEM((count, size, size), F32)
    tiles, new_state = pl.pallas_call(
        attention_kernel,
        out_shape=(
            pltpu.VMEM((tp, count, part), BF16),
            pltpu.HBM((count, size, size), F32),
        ),
        in_specs=[VMEM] * 11,
        out_specs=(VMEM, HBM),
        scratch_shapes=[
            pltpu.VMEM((count, width), BF16),
            pltpu.VMEM((count, size), F32),
            pltpu.VMEM((count, size), F32),
            states,
            pltpu.SemaphoreType.DMA((4,)),
        ],
        compiler_params=pltpu.CompilerParams(vmem_limit_bytes=16 << 20),
        name="attention",
    )(
        tiles,
        attn_gain.reshape(1, width),
        w_rates.reshape(2, width),
        rate_row,
        head_gain.reshape(1, size),
        *in_vmem(
            w_query, w_key, w_value, w_outgate, w_out, state.reshape(count, size, size)
        ),
    )
    tiles = lax.all_to_all(tiles, "tp", 0, 0, tiled=True, axis_index_groups=ring)
    half_count = count // 2
    residual, blocks = pl.pallas_call(
        functools.partial(residual_kernel, order),
        out_shape=(
            pltpu.VMEM((count, part), BF16),
            pltpu.VMEM((peers, half_count, part), BF16),
        ),
        in_specs=[VMEM, VMEM],
        out_specs=(VMEM, VMEM),
        compiler_params=pltpu.CompilerParams(vmem_limit_bytes=4 << 20),
        name="residual",
    )(tiles, kept)

    blocks, above, below = lax.optimization_barrier((blocks, above, below))
    far = lax.ppermute(above, ("kv", "tp"), y_ring(1, side, tp))
    above_2 = lax.ppermute(above, "tp", partner)
    below_2 = lax.ppermute(below, "tp", partner)
    tiles = lax.all_to_all(
        blocks, ("kv", "tp"), 0, 0, tiled=True, axis_index_groups=groups
    )
    tiles, far = lax.optimization_barrier((tiles, far))
    rows = side * half_count
    far_2 = lax.ppermute(far, "tp", partner)
    xn, near = pl.pallas_call(
        functools.partial(near_kernel, side, order),
        out_shape=(pltpu.VMEM((rows, width), BF16), pltpu.VMEM((rows, width), F32)),
        in_specs=[VMEM] * 9,
        out_specs=(VMEM, VMEM),
        compiler_params=pltpu.CompilerParams(vmem_limit_bytes=8 << 20),
        cost_estimate=pl.CostEstimate(
            flops=8_000_000_000, bytes_accessed=8_000_000, transcendentals=0
        ),
        name="near",
    )(
        tiles,
        mlp_gain.reshape(1, width),
        *in_vmem(own, above, below, own_2, above_2, below_2, far),
    )
    tiles = pl.pallas_call(
        functools.partial(far_kernel, side, order),
        out_shape=pltpu.VMEM((peers, half_count, part), BF16),
        in_specs=[VMEM] * 3,
        out_specs=VMEM,
        compiler_params=pltpu.CompilerParams(vmem_limit_bytes=8 << 20),
        name="far",
    )(xn, near, *in_vmem(far_2))
    tiles = lax.all_to_all(
        tiles, ("kv", "tp"), 0, 0, tiled=True, axis_index_groups=groups
    )
    result = pl.pallas_call(
        functools.partial(last_kernel, order),
        out_shape=jax.ShapeDtypeStruct((count, part), BF16),
        in_specs=[VMEM] * 2,
        out_specs=VMEM,
        compiler_params=pltpu.CompilerParams(vmem_limit_bytes=1 << 20),
        name="last",
    )(tiles, residual)
    return (result, new_state[:, None])


def solution(mesh):
    return jax.shard_map(
        body,
        mesh=mesh,
        in_specs=(
            P("kv", "tp"),
            P(),
            P(None, "tp"),
            P(None, "tp"),
            P(None, "tp"),
            P(None, "tp"),
            P(None, None, "tp"),
            P("tp"),
            P("tp"),
            P("tp", None),
            P("kv", "tp", None, None),
            P(),
            P(None, ("kv", "tp")),
            P(None, ("kv", "tp")),
            P(None, ("kv", "tp")),
        ),
        out_specs=(P("kv", "tp"), P("kv", "tp", None, None)),
        check_vma=False,
    )
```
